32 devices in a mesh: kv: 8 (over z, x), tp: 4 (over y, core).
Axes of the slice: x: 2, y: 2, z: 4, core: 2. Of those that a mesh axis runs over, the one named last changes fastest.
Arguments:
- tokens: bfloat16 [256, 4096], P(None, ('kv', 'tp')), may hold values from -6 to 6
- previous_state: float32 [256, 32, 128, 128], P('kv', 'tp'), may hold values from -6 to 6
- lengths: int32 [256], P('kv'), may hold values from 1 to 16384, 1048576 in all
- first_feed_norm_gain: float32 [4096], replicated, may hold values from 0.1 to 1.9
- first_gate_projection: bfloat16 [4096, 11264], P('kv', 'tp'), may hold values from -0.09375 to 0.09375
- first_up_projection: bfloat16 [4096, 11264], P('kv', 'tp'), may hold values from -0.09375 to 0.09375
- first_down_projection: bfloat16 [11264, 4096], P('tp', 'kv'), may hold values from -0.078125 to 0.078125
- mixer_norm_gain: float32 [4096], replicated, may hold values from 0.1 to 1.9
- query_weight: bfloat16 [4096, 4096], P('kv', 'tp'), may hold values from -0.09375 to 0.09375
- key_weight: bfloat16 [4096, 4096], P('kv', 'tp'), may hold values from -0.09375 to 0.09375
- value_weight: bfloat16 [4096, 4096], P('kv', 'tp'), may hold values from -0.09375 to 0.09375
- output_gate_weight: bfloat16 [4096, 4096], P('kv', 'tp'), may hold values from -0.09375 to 0.09375
- write_strength_weight: bfloat16 [4096, 32], replicated, may hold values from -0.09375 to 0.09375
- decay_input_weight: bfloat16 [4096, 32], replicated, may hold values from -0.09375 to 0.09375
- head_log_decay_rate: float32 [32], P('tp'), may hold values from -5 to 1
- decay_input_bias: float32 [32], P('tp'), may hold values from -1 to 1
- length_span_bias: float32 [32, 17], P('tp'), may hold values from -2 to 2
- extra_log_decay: float32 [256, 32], P('kv', 'tp'), may hold values from -0.7 to 0
- readout_head_norm_gain: float32 [128], replicated, may hold values from 0.1 to 1.9
- mixer_output_weight: bfloat16 [4096, 4096], P('tp', 'kv'), may hold values from -0.125 to 0.125
- second_feed_norm_gain: float32 [4096], replicated, may hold values from 0.1 to 1.9
- second_gate_projection: bfloat16 [4096, 11264], P('kv', 'tp'), may hold values from -0.09375 to 0.09375
- second_up_projection: bfloat16 [4096, 11264], P('kv', 'tp'), may hold values from -0.09375 to 0.09375
- second_down_projection: bfloat16 [11264, 4096], P('tp', 'kv'), may hold values from -0.078125 to 0.078125
Outputs:
- result: bfloat16 [256, 4096], P(None, ('kv', 'tp'))
- new_state: float32 [256, 32, 128, 128], P('kv', 'tp')
The draws below stay inside these ranges and needn't reach their ends.
All inputs are finite; a program needn't handle non-finite values. No bound on the sum of `lengths` on one device may be relied on, other than what follows from the above.
Results may differ from the reference program's by a relative error of at most 0.03.
Values may be sent and summed in bfloat16 or wider, within the bound.
A program may use at most 128 MiB of HBM per device.

```python
import math
import jax
import jax.numpy as jnp
import numpy as np
from jax import lax

D = 4096
HEADS = 32
HEAD = 128
FF = 11264
LEN_MEAN = 4096
MAX_LEN = 16384
SPAN = 1024
POS_BLOCKS = 17
SEQS = 256


def draw_tokens(key, part):
    column = jnp.arange(D, dtype=jnp.float32) / D
    col_scale = 0.3 * jnp.exp(math.log(3.0) * column)
    values = jax.random.normal(key, (SEQS, D), jnp.float32) * col_scale
    return jnp.clip(values, -6.0, 6.0).astype(jnp.bfloat16)


def draw_head_log_decay_rate(key, part):
    values = jax.random.uniform(key, (HEADS,), jnp.float32, -4.0, 1.0)
    return values.astype(jnp.float32)


def draw_extra_log_decay(key, part):
    chance = 0.25
    hits = jax.random.bernoulli(jax.random.fold_in(key, 21), chance, (SEQS, HEADS))
    depth = jax.random.uniform(jax.random.fold_in(key, 22), (SEQS, HEADS), jnp.float32, 0.22, 0.7)
    return jnp.where(hits, -depth, 0.0).astype(jnp.float32)


def spiked(values, key, source, target, parts, factor):
    owner, partner = [(jnp.arange(values.shape[position]) // (values.shape[position] // parts)).reshape([-1 if axis == position else 1 for axis in range(values.ndim)]) for position in (source, target)]
    chosen = jax.random.permutation(key, parts)[partner]
    strong = (owner == chosen) | (owner == (partner + parts // 2) % parts)
    return jnp.where(strong, factor * values, values)


def levels(rng, dims, shards, least, largest):
    level, own = 1.0, jax.random.fold_in(rng, 6)
    for position, parts in shards:
        heights = jnp.exp(jax.random.uniform(jax.random.fold_in(own, position), (parts,), jnp.float32, least / len(shards), largest / len(shards)))
        level = level * jnp.repeat(heights, dims[position] // parts).reshape([-1 if axis == position else 1 for axis in range(len(dims))])
    return level


def split_up(amount, total, limit, slope):
    portions = [(1 << 20) // math.isqrt(grade ** slope) + 1 for grade in range(2, amount + 1)]
    spare, holding = total - limit - (amount - 1), [1] * (amount - 1)
    while spare > 0:
        movable = [i for i in range(amount - 1) if holding[i] < limit]
        whole, remaining = sum([portions[i] for i in movable]), spare
        for i in movable:
            more = min(limit - holding[i], max(1, remaining * portions[i] // whole), spare)
            holding[i] = holding[i] + more
            spare = spare - more
    return np.array([limit] + holding)


def ragged(stream_key, count, total, bound, lean):
    if count == 2:
        one = jax.random.randint(stream_key, (), max(1, total - bound), min(bound, total - 1) + 1)
        return jnp.stack([one, total - one])
    sizes = jnp.asarray(split_up(count, total, bound, lean), jnp.int32)
    couples = (count - 1) // 2
    source_of, sink = sizes[1:1 + 2 * couples:2], sizes[2:2 + 2 * couples:2]
    room = jnp.minimum(source_of - 1, bound - sink)
    moved = jax.random.randint(jax.random.fold_in(stream_key, 1), (couples,), 0, 1 << 20) % (room + 1)
    sizes = sizes.at[1:1 + 2 * couples:2].set(source_of - moved).at[2:2 + 2 * couples:2].set(sink + moved)
    return sizes[jax.random.permutation(jax.random.fold_in(stream_key, 2), count)]


def scatter_about(stream_key, dims, width, bound, split=(), kind=jnp.bfloat16):
    factor_of = levels(stream_key, dims, split, -0.22, 0.18) if split else 1.0
    entries = jax.random.normal(stream_key, dims, jnp.float32) * width * factor_of
    return jnp.minimum(jnp.maximum(entries, -bound), bound).astype(kind)


def bell_draw_with(stream_key, extent, width, most, shards, heavy, kind=jnp.bfloat16):
    drawn = width * jax.random.normal(stream_key, extent, jnp.float32)
    if shards:
        drawn = drawn * levels(stream_key, extent, shards, -0.22, 0.18)
    return jnp.clip(spiked(drawn, jax.random.fold_in(stream_key, 3), *heavy), -most, most).astype(kind)


def setup_inputs(seed: int = 0) -> dict:
    seeds = jax.random.split(jax.random.key(seed), 25)
    return {
        "tokens": draw_tokens(jax.random.fold_in(seeds[24], 71), 0),
        "previous_state": scatter_about(seeds[1], (SEQS, HEADS, HEAD, HEAD), 1.0, 6.0, ((0, 8), (1, 4)), jnp.float32),
        "lengths": ragged(seeds[2], SEQS, SEQS * LEN_MEAN, MAX_LEN, 2).astype(jnp.int32),
        "first_feed_norm_gain": jnp.clip(1.0 + 0.18 * jax.random.normal(seeds[3], (D,), jnp.float32), 0.1, 1.9),
        "first_gate_projection": scatter_about(seeds[4], (D, FF), D ** -0.5, 0.09375, ((0, 8), (1, 4))),
        "first_up_projection": scatter_about(seeds[5], (D, FF), D ** -0.5, 0.09375, ((0, 8), (1, 4))),
        "first_down_projection": bell_draw_with(seeds[6], (FF, D), FF ** -0.5, 0.078125, ((0, 4), (1, 8)), (0, 1, 8, 2.0)),
        "mixer_norm_gain": jnp.clip(1.0 + 0.18 * jax.random.normal(seeds[7], (D,), jnp.float32), 0.1, 1.9),
        "query_weight": scatter_about(seeds[8], (D, HEADS * HEAD), D ** -0.5, 0.09375, ((0, 8), (1, 4))),
        "key_weight": scatter_about(seeds[9], (D, HEADS * HEAD), D ** -0.5, 0.09375, ((0, 8), (1, 4))),
        "value_weight": scatter_about(seeds[10], (D, HEADS * HEAD), D ** -0.5, 0.09375, ((0, 8), (1, 4))),
        "output_gate_weight": scatter_about(seeds[11], (D, HEADS * HEAD), D ** -0.5, 0.09375, ((0, 8), (1, 4))),
        "write_strength_weight": scatter_about(seeds[12], (D, HEADS), D ** -0.5, 0.09375),
        "decay_input_weight": scatter_about(seeds[13], (D, HEADS), D ** -0.5, 0.09375),
        "head_log_decay_rate": draw_head_log_decay_rate(jax.random.fold_in(seeds[24], 71), 0),
        "decay_input_bias": jnp.clip(jax.random.uniform(seeds[15], (HEADS,), jnp.float32, -1.0, 1.0) * levels(seeds[15], (HEADS,), ((0, 4),), -0.4, 0.0), -1.0, 1.0),
        "length_span_bias": jnp.clip(jax.random.uniform(seeds[16], (HEADS, POS_BLOCKS), jnp.float32, -2.0, 2.0) * levels(seeds[16], (HEADS, POS_BLOCKS), ((0, 4),), -0.4, 0.0), -2.0, 2.0),
        "extra_log_decay": draw_extra_log_decay(jax.random.fold_in(seeds[24], 71), 0),
        "readout_head_norm_gain": jnp.clip(1.0 + 0.18 * jax.random.normal(seeds[18], (HEAD,), jnp.float32), 0.1, 1.9),
        "mixer_output_weight": bell_draw_with(seeds[19], (HEADS * HEAD, D), (HEADS * HEAD) ** -0.5, 0.125, ((0, 4), (1, 8)), (0, 1, 8, 2.0)),
        "second_feed_norm_gain": jnp.clip(1.0 + 0.18 * jax.random.normal(seeds[20], (D,), jnp.float32), 0.1, 1.9),
        "second_gate_projection": scatter_about(seeds[21], (D, FF), D ** -0.5, 0.09375, ((0, 8), (1, 4))),
        "second_up_projection": scatter_about(seeds[22], (D, FF), D ** -0.5, 0.09375, ((0, 8), (1, 4))),
        "second_down_projection": bell_draw_with(seeds[23], (FF, D), FF ** -0.5, 0.078125, ((0, 4), (1, 8)), (0, 1, 8, 2.0)),
    }


EPSILON = 1e-06

def rms_rows(stream):
    values = stream.astype(jnp.float32)
    return lax.rsqrt(lax.optimization_barrier(jnp.mean(values * values, axis=-1, keepdims=True)) + EPSILON)

def half_ffn(stream, gain, w_gate, w_up, w_down):
    row_scale = rms_rows(stream)
    scaled = (stream.astype(jnp.float32) * gain).astype(jnp.bfloat16)
    gate_vals = row_scale * jnp.dot(scaled, w_gate, preferred_element_type=jnp.float32)
    up_vals = row_scale * jnp.dot(scaled, w_up, preferred_element_type=jnp.float32)
    hidden = (jax.nn.silu(gate_vals) * up_vals).astype(jnp.bfloat16)
    return jnp.dot(hidden, w_down, preferred_element_type=jnp.float32)

def unit_heads(raw):
    return raw * lax.rsqrt(lax.optimization_barrier(jnp.sum(raw * raw, axis=-1, keepdims=True)) + EPSILON)

def reference(tokens, previous_state, lengths, first_feed_norm_gain, first_gate_projection, first_up_projection, first_down_projection, mixer_norm_gain, query_weight, key_weight, value_weight, output_gate_weight, write_strength_weight, decay_input_weight, head_log_decay_rate, decay_input_bias, length_span_bias, extra_log_decay, readout_head_norm_gain, mixer_output_weight, second_feed_norm_gain, second_gate_projection, second_up_projection, second_down_projection):
    first = (tokens.astype(jnp.float32) + 0.5 * half_ffn(tokens, first_feed_norm_gain, first_gate_projection, first_up_projection, first_down_projection)).astype(jnp.bfloat16)
    row_scale = rms_rows(first)
    scaled = (first.astype(jnp.float32) * mixer_norm_gain).astype(jnp.bfloat16)

    def apply_projection(weight):
        return row_scale * jnp.dot(scaled, weight, preferred_element_type=jnp.float32)

    def split_heads(raw):
        return raw.reshape(SEQS, HEADS, HEAD)
    queries = unit_heads(jax.nn.silu(split_heads(apply_projection(query_weight)))) * HEAD ** (-0.5)
    key_heads = unit_heads(jax.nn.silu(split_heads(apply_projection(key_weight))))
    value_heads = jax.nn.silu(split_heads(apply_projection(value_weight)))
    out_gate = jax.nn.silu(split_heads(apply_projection(output_gate_weight)))
    beta_gate = jax.nn.sigmoid(apply_projection(write_strength_weight))
    span_index = (lengths // SPAN).astype(jnp.int32)
    span_decay_bias = jnp.take(length_span_bias, span_index, axis=1).T
    decay_logarithm = -jnp.exp(head_log_decay_rate) * jax.nn.softplus(apply_projection(decay_input_weight) + decay_input_bias + span_decay_bias) + extra_log_decay
    held_state = jnp.exp(decay_logarithm)[..., None, None] * previous_state
    predicted = jnp.einsum('bhkv,bhk->bhv', held_state, key_heads, precision=lax.Precision.HIGHEST)
    new_state = held_state + beta_gate[..., None, None] * key_heads[..., None] * (value_heads - predicted)[..., None, :]
    readout = jnp.einsum('bhkv,bhk->bhv', new_state, queries, precision=lax.Precision.HIGHEST)
    readout = readout * lax.rsqrt(lax.optimization_barrier(jnp.mean(readout * readout, axis=-1, keepdims=True)) + EPSILON) * readout_head_norm_gain * out_gate
    mixed = readout.reshape(SEQS, HEADS * HEAD).astype(jnp.bfloat16)
    second = (first.astype(jnp.float32) + jnp.dot(mixed, mixer_output_weight, preferred_element_type=jnp.float32)).astype(jnp.bfloat16)
    result = (second.astype(jnp.float32) + 0.5 * half_ffn(second, second_feed_norm_gain, second_gate_projection, second_up_projection, second_down_projection)).astype(jnp.bfloat16)
    return (result, new_state)
```

```python
import functools
from types import SimpleNamespace

import jax
import jax.numpy as jnp
from jax import lax
from jax.experimental import pallas as pl
from jax.experimental.pallas import tpu as pltpu
from jax.sharding import PartitionSpec as P

SPAN = 1024


EPSILON = 1e-06


LANES = 128


LIMIT = 46 << 20


KV = "kv"


TP = "tp"


MESH = pl.DeviceIdType.MESH


def log2(n):
    return n.bit_length() - 1


def bit(value, place):
    return lax.rem(value // (1 << place), 2)


def orders(n):
    bits = log2(n)
    plain = tuple(range(bits))
    swapped = (1, 0) + tuple(range(2, bits)) if bits > 1 else plain
    return plain, swapped


def place_of(block, order):
    bits = len(order)
    return sum(((block >> b) & 1) << (bits - 1 - k) for k, b in enumerate(order))


def meet(kv, tp, n_kv, n_tp):
    barrier = pltpu.get_barrier_semaphore()
    for away in range(1, n_kv):
        pl.semaphore_signal(
            barrier, inc=1, device_id={KV: lax.rem(kv + away, n_kv)}, device_id_type=MESH
        )
    for away in range(1, n_tp):
        pl.semaphore_signal(
            barrier, inc=1, device_id={TP: lax.rem(tp + away, n_tp)}, device_id_type=MESH
        )
    pl.semaphore_wait(barrier, n_kv + n_tp - 2)


def to_kv(src, dst, send, recv, peer):
    return pltpu.make_async_remote_copy(
        src_ref=src,
        dst_ref=dst,
        send_sem=send,
        recv_sem=recv,
        device_id={KV: peer},
        device_id_type=MESH,
    )


def to_tp(src, dst, send, recv, peer):
    return pltpu.make_async_remote_copy(
        src_ref=src,
        dst_ref=dst,
        send_sem=send,
        recv_sem=recv,
        device_id={TP: peer},
        device_id_type=MESH,
    )


def sum_rows_start(refs, kv, n):
    copies = []
    for away in range(1, n):
        peer = lax.rem(kv + away, n)
        copy = to_kv(
            refs.row_part.at[peer],
            refs.row_slot.at[away - 1],
            refs.row_sem.at[0, away - 1],
            refs.row_sem.at[1, away - 1],
            peer,
        )
        copy.start()
        copies.append(copy)
    return copies


def sum_rows_finish(refs, copies, kv, n):
    for copy in copies:
        copy.wait_recv()
    total = refs.row_part[kv]
    for away in range(n - 1):
        total = total + refs.row_slot[away]
    return total


class Exchange:
    def __init__(self, refs, kv, n, chunks, plain_chunks):
        self.refs, self.kv, self.n = refs, kv, n
        self.chunks, self.plain_chunks = chunks, plain_chunks
        self.bits = log2(n)
        self.orders = orders(n)

    def mine(self, j, k):
        first, second = self.orders[0][k], self.orders[1][k]
        if first == second:
            return bit(self.kv, first)
        return jnp.where(j < self.plain_chunks, bit(self.kv, first), bit(self.kv, second))

    def peer(self, j, k):
        first, second = self.orders[0][k], self.orders[1][k]
        up = self.kv + (1 - 2 * bit(self.kv, first)) * (1 << first)
        if first == second:
            return up
        other = self.kv + (1 - 2 * bit(self.kv, second)) * (1 << second)
        return jnp.where(j < self.plain_chunks, up, other)

    def place(self, depth):
        total = 0
        for k in range(depth):
            total = total + bit(self.kv, k) * (self.n >> (k + 1))
        return total

    def scatter(self, j, k):
        return to_kv(
            self.refs.part[k].at[j, 1 - self.mine(j, k)],
            self.refs.slot[k].at[j],
            self.refs.scatter_sem.at[0, k, j],
            self.refs.scatter_sem.at[1, k, j],
            self.peer(j, k),
        )

    def gather(self, j, a):
        last = self.bits - 1 - a
        window = self.refs.full.at[j, pl.ds(self.place(self.bits - a), 1 << a)]
        return to_kv(
            window,
            window,
            self.refs.gather_sem.at[0, a, j],
            self.refs.gather_sem.at[1, a, j],
            self.kv + (1 - 2 * bit(self.kv, last)) * (1 << last),
        )

    def produce(self, product):
        rows = self.refs.slot[-1].shape[1]
        part = self.refs.part[0]
        half = self.n // 2
        for order, low, high in (
            (self.orders[0], 0, 1),
            (self.orders[1], self.plain_chunks, self.chunks),
            (self.orders[0], 1, self.plain_chunks),
        ):

            def step(j, carry, order=order):
                value = product(j)
                for block in range(self.n):
                    place = place_of(block, order)
                    start = (place % half) * rows
                    part[j, place // half, start : start + rows] = value[
                        block * rows : (block + 1) * rows
                    ].astype(part.dtype)
                self.scatter(j, 0).start()
                return carry

            if high > low:
                lax.fori_loop(low, high, step, 0)

    def reduce(self, j, k, finish):
        self.scatter(j, k - 1).wait_recv()
        total = self.refs.part[k - 1][j, self.mine(j, k - 1)].astype(jnp.float32)
        total = total + self.refs.slot[k - 1][j].astype(jnp.float32)
        if k < self.bits:
            part = self.refs.part[k]
            rows = total.shape[0] // 2
            part[j, 0] = total[:rows].astype(part.dtype)
            part[j, 1] = total[rows:].astype(part.dtype)
            self.scatter(j, k).start()
        else:
            full = self.refs.full
            full[j, self.place(self.bits)] = finish(j, total)
            self.gather(j, 0).start()

    def relay(self, j, a):
        self.gather(j, a - 1).wait_recv()
        self.gather(j, a).start()

    def run(self, finish):
        bits = self.bits

        def step(t, carry):
            @pl.when(t < self.plain_chunks)
            def _():
                self.reduce(t, 1, finish)

            @pl.when(t < self.chunks - self.plain_chunks)
            def _():
                self.reduce(self.plain_chunks + t, 1, finish)

            for lag in range(1, 2 * bits - 1):
                j = t - lag

                @pl.when(jnp.logical_and(j >= 0, j < self.chunks))
                def _(lag=lag, j=j):
                    if lag < bits:
                        self.reduce(j, lag + 1, finish)
                    else:
                        self.relay(j, lag - bits + 1)

            return carry

        lax.fori_loop(0, self.chunks + 2 * bits - 2, step, 0)

    def consume(self, total, weight, weight_wait):
        full = self.refs.full
        rows, width = full.shape[2], full.shape[3]
        total[...] = jnp.zeros_like(total)
        order = self.orders[0]

        def step(j, carry):
            weight_wait(j)
            self.gather(j, self.bits - 1).wait_recv()
            product = jnp.dot(
                full[j].reshape(self.n * rows, width),
                weight[j],
                preferred_element_type=jnp.float32,
            )
            for block in range(self.n):
                place = place_of(block, order)
                total[block * rows : (block + 1) * rows] += product[
                    place * rows : (place + 1) * rows
                ]
            return carry

        lax.fori_loop(0, self.chunks, step, 0)

    def drain(self):
        def step(j, carry):
            for k in range(self.bits):
                self.scatter(j, k).wait_send()
                self.gather(j, k).wait_send()
            return carry

        lax.fori_loop(0, self.chunks, step, 0)


def total_over_tp(refs, total, base, out, scale, tp, n_tp):
    half = total.shape[0] // 2
    core = bit(tp, 0)
    other = tp + 1 - 2 * core
    part, slot, sems = refs.tp_part, refs.tp_slot, refs.tp_sem
    part[0, 0] = total[:half].astype(part.dtype)
    part[0, 1] = total[half:].astype(part.dtype)
    copies = [to_tp(part.at[0, 1 - core], slot.at[0], sems.at[0, 0], sems.at[1, 0], other)]
    copies[-1].start()
    copies[-1].wait_recv()
    value = part[0, core].astype(jnp.float32) + slot[0].astype(jnp.float32)
    for place in range(1, log2(n_tp)):
        part[place, 0] = value.astype(part.dtype)
        peer = tp + (1 - 2 * bit(tp, place)) * (1 << place)
        copies.append(
            to_tp(part.at[place, 0], slot.at[place], sems.at[0, place], sems.at[1, place], peer)
        )
        copies[-1].start()
        copies[-1].wait_recv()
        value = part[place, 0].astype(jnp.float32) + slot[place].astype(jnp.float32)
    out[core] = (base[core].astype(jnp.float32) + scale * value).astype(out.dtype)
    last = log2(n_tp)
    copies.append(to_tp(out.at[core], out.at[core], sems.at[0, last], sems.at[1, last], other))
    copies[-1].start()
    copies[-1].wait_recv()
    return copies


def exchange_scratch(n, chunks, rows, cols, width):
    bits = log2(n)
    shapes = SimpleNamespace()
    shapes.part = [
        pltpu.VMEM((chunks, 2, rows >> (k + 1), cols), jnp.bfloat16) for k in range(bits)
    ]
    shapes.slot = [
        pltpu.VMEM((chunks, rows >> (k + 1), cols), jnp.bfloat16) for k in range(bits)
    ]
    shapes.full = pltpu.VMEM((chunks, n, rows // n, width), jnp.bfloat16)
    shapes.scatter_sem = pltpu.SemaphoreType.DMA((2, bits, chunks))
    shapes.gather_sem = pltpu.SemaphoreType.DMA((2, bits, chunks))
    shapes.row_part = pltpu.VMEM((n, rows // n, LANES), jnp.float32)
    shapes.row_slot = pltpu.VMEM((n - 1, rows // n, LANES), jnp.float32)
    shapes.row_sem = pltpu.SemaphoreType.DMA((2, n - 1))
    return shapes


def tp_scratch(n_tp, rows, cols):
    bits = log2(n_tp)
    return dict(
        tp_part=pltpu.VMEM((bits, 2, rows // 2, cols), jnp.bfloat16),
        tp_slot=pltpu.VMEM((bits, rows // 2, cols), jnp.bfloat16),
        tp_sem=pltpu.SemaphoreType.DMA((2, bits + 1)),
    )


def chunks_of(columns):
    tiles = columns // LANES
    return max(d for d in range(1, 13) if tiles % d == 0)


def plain_share(n, chunks):
    return chunks if log2(n) < 2 else chunks - (chunks + 2) // 6


def scale_rows(x, gain, scaled, kv):
    half, cols = x.shape[1:]
    columns = gain[:, pl.ds(pl.multiple_of(kv * cols, LANES), cols)]
    squares = []
    for side in range(2):
        values = x[side].astype(jnp.float32)
        squares.append(jnp.sum(values * values, axis=1, keepdims=True))
        scaled[side * half : (side + 1) * half] = (values * columns).astype(jnp.bfloat16)
    return jnp.concatenate(squares, axis=0)


class Feed:
    def __init__(self, refs, sources, kv, tp):
        self.refs, self.sources, self.kv, self.tp = refs, sources, kv, tp
        self.n, self.n_tp = lax.axis_size(KV), lax.axis_size(TP)
        self.chunks, self.width = refs.down.shape[:2]

    def fetch(self, j, side):
        columns = pl.ds(pl.multiple_of(j * self.width, LANES), self.width)
        return pltpu.make_async_copy(
            self.sources[side].at[:, columns],
            self.refs.weights.at[j, :, pl.ds(side * self.width, self.width)],
            self.refs.weight_sem.at[side, j],
        )

    def fetch_down(self, j):
        return pltpu.make_async_copy(
            self.sources[2].at[pl.ds(pl.multiple_of(j * self.width, LANES), self.width)],
            self.refs.down.at[j],
            self.refs.weight_sem.at[2, j],
        )

    def start_weights(self):
        def step(j, carry):
            self.fetch(j, 0).start()
            self.fetch(j, 1).start()
            return carry

        lax.fori_loop(0, self.chunks, step, 0)

    def start_down(self):
        def step(j, carry):
            self.fetch_down(j).start()
            return carry

        lax.fori_loop(0, self.chunks, step, 0)

    def run(self, x, gain, model_width):
        refs, kv, n, width = self.refs, self.kv, self.n, self.width
        squares = scale_rows(x, gain, refs.scaled, kv)
        rows = squares.shape[0]
        refs.row_part[...] = jnp.broadcast_to(squares, (rows, LANES)).reshape(
            n, rows // n, LANES
        )
        row_copies = sum_rows_start(refs, kv, n)
        exchange = Exchange(refs, kv, n, self.chunks, plain_share(n, self.chunks))

        def product(j):
            self.fetch(j, 0).wait()
            self.fetch(j, 1).wait()
            return jnp.dot(
                refs.scaled[...], refs.weights[j], preferred_element_type=jnp.float32
            )

        exchange.produce(product)
        totals = sum_rows_finish(refs, row_copies, kv, n)
        refs.row_scale[...] = lax.rsqrt(totals / model_width + EPSILON)

        def finish(j, sums):
            row_scale = refs.row_scale[:, :1]
            gate = row_scale * sums[:, :width]
            up = row_scale * sums[:, width:]
            return (jax.nn.silu(gate) * up).astype(jnp.bfloat16)

        exchange.run(finish)
        exchange.consume(refs.total, refs.down, lambda j: self.fetch_down(j).wait())

        def drain():
            exchange.drain()
            for copy in row_copies:
                copy.wait_send()

        return drain


def own_columns(refs, total, base, out, tp, n_tp):
    part, slot, sems = refs.out_part, refs.out_slot, refs.out_sem
    rows, own = part.shape[1:]
    half = rows // 2
    for piece in range(n_tp):
        part[piece] = total[:, piece * own : (piece + 1) * own].astype(part.dtype)
    copies = []
    for away in range(1, n_tp):
        peer = lax.rem(tp + away, n_tp)
        copy = to_tp(
            part.at[peer], slot.at[away - 1], sems.at[0, away - 1], sems.at[1, away - 1], peer
        )
        copy.start()
        copies.append(copy)
    value = part[tp].astype(jnp.float32)
    for away in range(1, n_tp):
        copies[away - 1].wait_recv()
        value = value + slot[away - 1].astype(jnp.float32)
    columns = pl.ds(pl.multiple_of(tp * own, LANES), own)
    for side in range(2):
        mine = base[side, :, columns].astype(jnp.float32)
        window = slice(side * half, (side + 1) * half)
        out[window] = (mine + 0.5 * value[window]).astype(out.dtype)
    return copies


class Mixer:
    def __init__(self, refs, io, kv, tp):
        self.refs, self.io, self.kv, self.tp = refs, io, kv, tp
        self.n, self.n_tp = lax.axis_size(KV), lax.axis_size(TP)
        self.heads, self.head_size, self.block_cols = refs.mix_out.shape
        self.slots = refs.state.shape[0]
        self.projections = (io.w_query, io.w_key, io.w_value, io.w_gate)

    def fetch(self, j, side):
        size = self.head_size
        return pltpu.make_async_copy(
            self.projections[side].at[:, pl.ds(pl.multiple_of(j * size, LANES), size)],
            self.refs.weights.at[j, :, pl.ds(side * size, size)],
            self.refs.weight_sem.at[side, j],
        )

    def fetch_mix(self, j):
        size = self.head_size
        return pltpu.make_async_copy(
            self.io.w_mix.at[pl.ds(pl.multiple_of(j * size, LANES), size)],
            self.refs.mix_out.at[j],
            self.refs.weight_sem.at[4, j],
        )

    def fetch_state(self, j):
        return pltpu.make_async_copy(
            self.io.previous.at[:, j],
            self.refs.state.at[lax.rem(j, self.slots)],
            self.refs.state_sem.at[j],
        )

    def fetch_small(self, side):
        start = pl.multiple_of(self.kv * self.block_cols, LANES)
        source = (self.io.w_beta, self.io.w_decay)[side]
        return pltpu.make_async_copy(
            source.at[:, pl.ds(start, self.block_cols)],
            self.refs.small_weights.at[side],
            self.refs.small_sem.at[side],
        )

    def start_fetches(self):
        self.fetch_small(0).start()
        self.fetch_small(1).start()

        def weights(j, carry):
            for side in range(4):
                self.fetch(j, side).start()
            self.fetch_mix(j).start()
            return carry

        def states(j, carry):
            self.fetch_state(j).start()
            return carry

        lax.fori_loop(0, self.heads, weights, 0)
        lax.fori_loop(0, self.slots, states, 0)

    def gates(self, totals, model_width):
        refs, io, heads = self.refs, self.io, self.heads
        all_heads = refs.small_weights.shape[1]
        block = totals.shape[0]
        row_scale = lax.rsqrt(
            totals[:, 2 * all_heads : 2 * all_heads + 1] / model_width + EPSILON
        )
        refs.row_scale[...] = jnp.broadcast_to(row_scale, (block, LANES))
        scaled_small = row_scale * totals
        lane = lax.broadcasted_iota(jnp.int32, (block, LANES), 1)
        own = lax.broadcasted_iota(jnp.int32, (block, block), 0) == lax.broadcasted_iota(
            jnp.int32, (block, block), 1
        )

        def stand(row):
            spread = jnp.broadcast_to(row, (block, block))
            return jnp.sum(jnp.where(own, spread, 0.0), axis=1, keepdims=True)

        span = jnp.floor(stand(io.lengths[...].astype(jnp.float32)) * (1.0 / SPAN))
        spans = io.span_bias.shape[1]
        matches = (
            lax.broadcasted_iota(jnp.int32, (block, spans), 1).astype(jnp.float32) == span
        )
        for h in range(heads):
            at = self.tp * heads + h
            beta_raw = jnp.sum(jnp.where(lane == at, scaled_small, 0.0), axis=1, keepdims=True)
            decay_raw = jnp.sum(
                jnp.where(lane == all_heads + at, scaled_small, 0.0), axis=1, keepdims=True
            )
            bias = jnp.sum(
                jnp.where(matches, io.span_bias[h : h + 1, :], 0.0), axis=1, keepdims=True
            )
            inner = decay_raw + io.decay_bias[:, h : h + 1] + bias
            soft = jnp.maximum(inner, 0.0) + jnp.log1p(jnp.exp(-jnp.abs(inner)))
            rate = jnp.exp(io.decay_rate[:, h : h + 1])
            decay = jnp.exp(-rate * soft + stand(io.extra[h : h + 1, :]))
            refs.decay[h] = jnp.broadcast_to(decay, (block, LANES))
            refs.beta[h] = jnp.broadcast_to(jax.nn.sigmoid(beta_raw), (block, LANES))

    def finish(self, j, sums):
        refs, io, size = self.refs, self.io, self.head_size
        block = sums.shape[0]

        def unit(raw):
            return raw * lax.rsqrt(jnp.sum(raw * raw, axis=1, keepdims=True) + EPSILON)

        sums = refs.row_scale[:, :1] * sums
        query = unit(jax.nn.silu(sums[:, :size])) * size ** (-0.5)
        key = unit(jax.nn.silu(sums[:, size : 2 * size]))
        value = jax.nn.silu(sums[:, 2 * size : 3 * size])
        gate = jax.nn.silu(sums[:, 3 * size :])
        refs.key[...] = key
        refs.value[...] = value
        refs.match[...] = jnp.broadcast_to(
            jnp.sum(key * query, axis=1, keepdims=True), (block, size)
        )
        refs.turned[...] = jnp.concatenate([key, query, value, gate], axis=0).T
        self.fetch_state(j).wait()
        slot = lax.rem(j, self.slots)
        for b in range(block):
            held = refs.state[slot, b]
            by_key = jnp.sum(held * refs.turned[:, b : b + 1], axis=0, keepdims=True)
            by_query = jnp.sum(
                held * refs.turned[:, block + b : block + b + 1], axis=0, keepdims=True
            )
            row = slice(b, b + 1)
            decay = refs.decay[j, row]
            write = refs.beta[j, row] * (refs.value[row] - decay * by_key)
            refs.readout[row] = decay * by_query + refs.match[row] * write
            io.decays[b, pl.ds(j, 1)] = decay
            io.keys[b, pl.ds(j, 1)] = refs.key[row]
            io.writes[b, pl.ds(j, 1)] = write

        @pl.when(j + self.slots < self.heads)
        def _():
            self.fetch_state(j + self.slots).start()

        readout = refs.readout[...]
        readout = (
            readout
            * lax.rsqrt(jnp.mean(readout * readout, axis=1, keepdims=True) + EPSILON)
            * io.head_gain[...]
            * gate
        )
        return readout.astype(jnp.bfloat16)

    def run(self, x, gain, model_width):
        refs, kv, n = self.refs, self.kv, self.n
        squares = scale_rows(x, gain, refs.scaled, kv)
        all_heads = refs.small_weights.shape[1]
        rows = squares.shape[0]
        small = refs.small
        small[...] = jnp.broadcast_to(squares, small.shape)
        for side in range(2):
            self.fetch_small(side).wait()
            small[:, side * all_heads : (side + 1) * all_heads] = lax.dot_general(
                refs.scaled[...],
                refs.small_weights[side],
                (((1,), (1,)), ((), ())),
                preferred_element_type=jnp.float32,
            )
        refs.row_part[...] = small[...].reshape(n, rows // n, LANES)
        row_copies = sum_rows_start(refs, kv, n)
        exchange = Exchange(refs, kv, n, self.heads, plain_share(n, self.heads))

        def product(j):
            for side in range(4):
                self.fetch(j, side).wait()
            return jnp.dot(
                refs.scaled[...], refs.weights[j], preferred_element_type=jnp.float32
            )

        exchange.produce(product)
        self.gates(sum_rows_finish(refs, row_copies, kv, n), model_width)
        exchange.run(self.finish)
        exchange.consume(refs.total, refs.mix_out, lambda j: self.fetch_mix(j).wait())

        def drain():
            exchange.drain()
            for copy in row_copies:
                copy.wait_send()

        return drain


def layer_kernel(model_width, aligned, io, refs):
    kv, tp = lax.axis_index(KV), lax.axis_index(TP)
    n, n_tp = lax.axis_size(KV), lax.axis_size(TP)
    feed, mix, blocks = refs.feed, refs.mix, refs.blocks
    half = blocks.shape[2]
    small_copies = []
    for item, (name, near) in enumerate(vars(refs.small).items()):
        copy = pltpu.make_async_copy(getattr(io, name), near, refs.small_sem.at[item])
        copy.start()
        small_copies.append(copy)
        setattr(io, name, near)
    if aligned:
        x_copies = [pltpu.make_async_copy(io.x, refs.pieces.at[tp], refs.x_sem.at[0])]
    else:
        x_copies = [
            pltpu.make_async_copy(
                io.x.at[pl.ds(side * half, half)], blocks.at[0, side], refs.x_sem.at[side]
            )
            for side in range(2)
        ]
    for copy in x_copies:
        copy.start()
    first = Feed(feed, (io.w_gate_one, io.w_up_one, io.w_down_one), kv, tp)
    second = Feed(feed, (io.w_gate_two, io.w_up_two, io.w_down_two), kv, tp)
    mixer = Mixer(mix, io, kv, tp)
    first.start_weights()
    meet(kv, tp, n, n_tp)
    for copy in x_copies:
        copy.wait()
    copies = []
    if aligned:
        own = io.x.shape[1]
        for away in range(1, n_tp):
            copy = to_tp(
                refs.pieces.at[tp],
                refs.pieces.at[tp],
                refs.piece_sem.at[0, away - 1],
                refs.piece_sem.at[1, away - 1],
                lax.rem(tp + away, n_tp),
            )
            copy.start()
            copies.append(copy)
    first.start_down()
    mixer.start_fetches()
    for copy in small_copies:
        copy.wait()
    for copy in copies:
        copy.wait_recv()
    if aligned:
        for piece in range(n_tp):
            columns = slice(piece * own, (piece + 1) * own)
            blocks[0, 0, :, columns] = refs.pieces[piece, :half]
            blocks[0, 1, :, columns] = refs.pieces[piece, half:]
    drain = first.run(blocks.at[0], io.gain_one, model_width)
    second.start_weights()
    second.start_down()
    copies += total_over_tp(
        refs.sums_one, feed.total, blocks.at[0], blocks.at[1], 0.5, tp, n_tp
    )
    drain_mixer = mixer.run(blocks.at[1], io.gain_mix, model_width)
    drain()
    copies += total_over_tp(refs.sums_mix, mix.total, blocks.at[1], blocks.at[2], 1.0, tp, n_tp)
    drain = second.run(blocks.at[2], io.gain_two, model_width)
    if aligned:
        copies += own_columns(refs, feed.total, blocks.at[2], io.out, tp, n_tp)
    else:
        copies += total_over_tp(refs.sums_two, feed.total, blocks.at[2], io.out, 0.5, tp, n_tp)
    drain()
    drain_mixer()
    for copy in copies:
        copy.wait_send()


def spaced(tree):
    if isinstance(tree, dict):
        return SimpleNamespace(**{name: spaced(leaf) for name, leaf in tree.items()})
    return tree


def call_kernel(kernel, inputs, outputs, scratch, name, call_id):
    arrays = [array for array, _ in inputs.values()]
    leaves, tree = jax.tree.flatten(scratch)

    def entry(*given):
        io = dict(zip([*inputs, *outputs], given))
        kernel(spaced(io), spaced(jax.tree.unflatten(tree, given[len(io) :])))

    return pl.pallas_call(
        entry,
        out_shape=[shape for shape, _ in outputs.values()],
        in_specs=[pl.BlockSpec(memory_space=space) for _, space in inputs.values()],
        out_specs=[pl.BlockSpec(memory_space=space) for _, space in outputs.values()],
        scratch_shapes=leaves,
        name=name,
        compiler_params=pltpu.CompilerParams(
            collective_id=call_id, has_side_effects=True, vmem_limit_bytes=LIMIT
        ),
    )(*arrays)


def row_scratch(scratch, rows, block_cols, n):
    scratch.scaled = pltpu.VMEM((rows, block_cols), jnp.bfloat16)
    scratch.row_scale = pltpu.VMEM((rows // n, LANES), jnp.float32)
    scratch.total = pltpu.VMEM((rows, block_cols), jnp.float32)
    return vars(scratch)


def layer(
    x,
    previous_state,
    lengths,
    gain_one,
    w_gate_one,
    w_up_one,
    w_down_one,
    gain_mix,
    w_query,
    w_key,
    w_value,
    w_gate,
    w_beta,
    w_decay,
    decay_rate,
    decay_bias,
    span_bias,
    extra,
    head_gain,
    w_mix,
    gain_two,
    w_gate_two,
    w_up_two,
    w_down_two,
    aligned,
):
    n, n_tp = lax.axis_size(KV), lax.axis_size(TP)
    rows = x.shape[0]
    block_cols, columns = w_gate_one.shape
    own = block_cols // n_tp
    block, heads, head_size = previous_state.shape[:3]
    all_heads = w_beta.shape[1]
    chunks = chunks_of(columns)
    width = columns // chunks
    vmem, hbm = pltpu.VMEM, pltpu.HBM

    def far(array):
        return (pltpu.with_memory_space_constraint(array, hbm), hbm)

    def row(array):
        return array.reshape(1, -1)

    small = dict(
        gain_one=row(gain_one),
        gain_mix=row(gain_mix),
        gain_two=row(gain_two),
        lengths=row(lengths),
        span_bias=span_bias,
        extra=extra.T,
        head_gain=row(head_gain),
        decay_rate=row(decay_rate),
        decay_bias=row(decay_bias),
    )
    inputs = dict(
        x=far(x),
        w_gate_one=far(w_gate_one),
        w_up_one=far(w_up_one),
        w_down_one=far(w_down_one),
        w_query=far(w_query),
        w_key=far(w_key),
        w_value=far(w_value),
        w_gate=far(w_gate),
        w_beta=far(w_beta.T),
        w_decay=far(w_decay.T),
        w_mix=far(w_mix),
        w_gate_two=far(w_gate_two),
        w_up_two=far(w_up_two),
        w_down_two=far(w_down_two),
        previous=far(previous_state),
        **{name: far(array) for name, array in small.items()},
    )
    shape = (rows, own) if aligned else (2, rows // 2, block_cols)
    rows_of_heads = jax.ShapeDtypeStruct((block, heads, head_size), jnp.float32)
    outputs = dict(
        out=(jax.ShapeDtypeStruct(shape, jnp.bfloat16), vmem),
        decays=(rows_of_heads, vmem),
        keys=(rows_of_heads, vmem),
        writes=(rows_of_heads, vmem),
    )
    feed = exchange_scratch(n, chunks, rows, 2 * width, width)
    feed.weights = vmem((chunks, block_cols, 2 * width), jnp.bfloat16)
    feed.down = vmem((chunks, width, block_cols), jnp.bfloat16)
    feed.weight_sem = pltpu.SemaphoreType.DMA((3, chunks))
    mix = exchange_scratch(n, heads, rows, 4 * head_size, head_size)
    mix.weights = vmem((heads, block_cols, 4 * head_size), jnp.bfloat16)
    mix.mix_out = vmem((heads, head_size, block_cols), jnp.bfloat16)
    mix.weight_sem = pltpu.SemaphoreType.DMA((5, heads))
    mix.state = vmem((min(heads, 4), block, head_size, head_size), jnp.float32)
    mix.state_sem = pltpu.SemaphoreType.DMA((heads,))
    mix.small_weights = vmem((2, all_heads, block_cols), jnp.bfloat16)
    mix.small_sem = pltpu.SemaphoreType.DMA((2,))
    mix.small = vmem((rows, LANES), jnp.float32)
    mix.decay = vmem((heads, block, LANES), jnp.float32)
    mix.beta = vmem((heads, block, LANES), jnp.float32)
    mix.key = vmem((block, head_size), jnp.float32)
    mix.value = vmem((block, head_size), jnp.float32)
    mix.match = vmem((block, head_size), jnp.float32)
    mix.readout = vmem((block, head_size), jnp.float32)
    mix.turned = vmem((head_size, 4 * block), jnp.float32)
    scratch = dict(
        feed=row_scratch(feed, rows, block_cols, n),
        mix=row_scratch(mix, rows, block_cols, n),
        blocks=vmem((3, 2, rows // 2, block_cols), jnp.bfloat16),
        sums_one=tp_scratch(n_tp, rows, block_cols),
        sums_mix=tp_scratch(n_tp, rows, block_cols),
        small={name: vmem(array.shape, array.dtype) for name, array in small.items()},
        small_sem=pltpu.SemaphoreType.DMA((len(small),)),
        x_sem=pltpu.SemaphoreType.DMA((2,)),
    )
    if aligned:
        scratch.update(
            pieces=vmem((n_tp, rows, own), jnp.bfloat16),
            piece_sem=pltpu.SemaphoreType.DMA((2, n_tp - 1)),
            out_part=vmem((n_tp, rows, own), jnp.bfloat16),
            out_slot=vmem((n_tp - 1, rows, own), jnp.bfloat16),
            out_sem=pltpu.SemaphoreType.DMA((2, n_tp - 1)),
        )
    else:
        scratch.update(sums_two=tp_scratch(n_tp, rows, block_cols))
    out, decays, keys, writes = call_kernel(
        functools.partial(layer_kernel, gain_one.shape[0], aligned),
        inputs,
        outputs,
        scratch,
        "layer",
        0,
    )
    return out if aligned else out.reshape(rows, block_cols), decays, keys, writes


def body(
    tokens,
    previous_state,
    lengths,
    first_feed_norm_gain,
    first_gate_projection,
    first_up_projection,
    first_down_projection,
    mixer_norm_gain,
    query_weight,
    key_weight,
    value_weight,
    output_gate_weight,
    write_strength_weight,
    decay_input_weight,
    head_log_decay_rate,
    decay_input_bias,
    length_span_bias,
    extra_log_decay,
    readout_head_norm_gain,
    mixer_output_weight,
    second_feed_norm_gain,
    second_gate_projection,
    second_up_projection,
    second_down_projection,
):
    own_cols = tokens.shape[1]
    aligned = own_cols % LANES == 0
    if not aligned:
        tokens = lax.all_gather(tokens, TP, axis=1, tiled=True)
    result, decays, keys, writes = layer(
        tokens,
        previous_state,
        lengths,
        first_feed_norm_gain,
        first_gate_projection,
        first_up_projection,
        first_down_projection,
        mixer_norm_gain,
        query_weight,
        key_weight,
        value_weight,
        output_gate_weight,
        write_strength_weight,
        decay_input_weight,
        head_log_decay_rate,
        decay_input_bias,
        length_span_bias,
        extra_log_decay,
        readout_head_norm_gain,
        mixer_output_weight,
        second_feed_norm_gain,
        second_gate_projection,
        second_up_projection,
        second_down_projection,
        aligned,
    )
    new_state = (
        decays[:, :, None, :] * previous_state + keys[:, :, :, None] * writes[:, :, None, :]
    )
    if not aligned:
        start = lax.axis_index(TP) * own_cols
        result = lax.dynamic_slice_in_dim(result, start, own_cols, 1)
    return (result, new_state)


def solution(mesh):
    return jax.shard_map(
        body,
        mesh=mesh,
        in_specs=(
            P(None, (KV, TP)),
            P(KV, TP, None, None),
            P(KV),
            P(),
            P(KV, TP),
            P(KV, TP),
            P(TP, KV),
            P(),
            P(KV, TP),
            P(KV, TP),
            P(KV, TP),
            P(KV, TP),
            P(),
            P(),
            P(TP),
            P(TP),
            P(TP, None),
            P(KV, TP),
            P(),
            P(TP, KV),
            P(),
            P(KV, TP),
            P(KV, TP),
            P(TP, KV),
        ),
        out_specs=(P(None, (KV, TP)), P(KV, TP, None, None)),
        check_vma=False,
    )
```

```python
import functools
from types import SimpleNamespace

import jax
import jax.numpy as jnp
from jax import lax
from jax.experimental import pallas as pl
from jax.experimental.pallas import tpu as pltpu
from jax.sharding import PartitionSpec as P

SPAN = 1024


EPSILON = 1e-06


LANES = 128


LIMIT = 46 << 20


PIECES = 2


KV = "kv"


TP = "tp"


MESH = pl.DeviceIdType.MESH


def log2(n):
    return n.bit_length() - 1


def bit(value, place):
    return lax.rem(value // (1 << place), 2)


def place_of(block, bits):
    return sum(((block >> k) & 1) << (bits - 1 - k) for k in range(bits))


def groups(n):
    near = max(n // 4, 2)
    return near, n // near


def meet(kv, tp, n_kv, n_tp):
    barrier = pltpu.get_barrier_semaphore()
    for away in range(1, n_kv):
        pl.semaphore_signal(
            barrier, inc=1, device_id={KV: lax.rem(kv + away, n_kv)}, device_id_type=MESH
        )
    for away in range(1, n_tp):
        pl.semaphore_signal(
            barrier, inc=1, device_id={TP: lax.rem(tp + away, n_tp)}, device_id_type=MESH
        )
    pl.semaphore_wait(barrier, n_kv + n_tp - 2)


def to_kv(src, dst, send, recv, peer):
    return pltpu.make_async_remote_copy(
        src_ref=src,
        dst_ref=dst,
        send_sem=send,
        recv_sem=recv,
        device_id={KV: peer},
        device_id_type=MESH,
    )


def to_tp(src, dst, send, recv, peer):
    return pltpu.make_async_remote_copy(
        src_ref=src,
        dst_ref=dst,
        send_sem=send,
        recv_sem=recv,
        device_id={TP: peer},
        device_id_type=MESH,
    )


def sum_rows_start(refs, kv, n):
    copies = []
    for away in range(1, n):
        peer = lax.rem(kv + away, n)
        copy = to_kv(
            refs.row_part.at[peer],
            refs.row_slot.at[away - 1],
            refs.row_sem.at[0, away - 1],
            refs.row_sem.at[1, away - 1],
            peer,
        )
        copy.start()
        copies.append(copy)
    return copies


def sum_rows_finish(refs, copies, kv, n):
    for copy in copies:
        copy.wait_recv()
    total = refs.row_part[kv]
    for away in range(n - 1):
        total = total + refs.row_slot[away]
    return total


class Exchange:
    def __init__(self, refs, kv, n, chunks):
        self.refs, self.chunks, self.kv, self.n = refs, chunks, kv, n
        self.bits = log2(n)
        self.near, self.far = groups(n)
        self.outer, self.inner = kv // self.near, lax.rem(kv, self.near)

    def inner_peer(self, away):
        return lax.rem(self.inner + away, self.near)

    def outer_peer(self, away):
        return sum(
            lax.rem(bit(self.outer, k) + (away >> k), 2) * (1 << k)
            for k in range(log2(self.far))
        )

    def scatter(self, j, k):
        side = bit(self.kv, k)
        return to_kv(
            self.refs.part[k].at[j, 1 - side],
            self.refs.slot[k].at[j],
            self.refs.scatter_sem.at[0, k, j],
            self.refs.scatter_sem.at[1, k, j],
            self.kv + (1 - 2 * side) * (1 << k),
        )

    def gather_far(self, j, away):
        own = self.refs.full.at[j, self.inner, self.outer]
        return to_kv(
            own,
            own,
            self.refs.back_sem.at[0, away - 1, j],
            self.refs.back_sem.at[1, away - 1, j],
            self.outer_peer(away) * self.near + self.inner,
        )

    def gather_near(self, j, away):
        window = self.refs.full.at[j, self.inner]
        return to_kv(
            window,
            window,
            self.refs.relay_sem.at[0, away - 1, j],
            self.refs.relay_sem.at[1, away - 1, j],
            self.outer * self.near + self.inner_peer(away),
        )

    def produce(self, product):
        part = self.refs.part[0]
        rows = self.refs.slot[-1].shape[1]
        half = self.n // 2

        def step(j, carry):
            value = product(j)
            for block in range(self.n):
                place = place_of(block, self.bits)
                start = place % half * rows
                part[j, place // half, start : start + rows] = value[
                    block * rows : (block + 1) * rows
                ].astype(part.dtype)
            self.scatter(j, 0).start()
            return carry

        lax.fori_loop(0, self.chunks, step, 0)

    def reduce(self, j, k, finish):
        self.scatter(j, k - 1).wait_recv()
        total = self.refs.part[k - 1][j, bit(self.kv, k - 1)].astype(jnp.float32)
        total = total + self.refs.slot[k - 1][j].astype(jnp.float32)
        if k < self.bits:
            part = self.refs.part[k]
            rows = total.shape[0] // 2
            part[j, 0] = total[:rows].astype(part.dtype)
            part[j, 1] = total[rows:].astype(part.dtype)
            self.scatter(j, k).start()
            return
        self.refs.full[j, self.inner, self.outer] = finish(j, total)
        for away in range(1, self.far):
            self.gather_far(j, away).start()

    def relay(self, j):
        for back in range(1, self.far):
            self.gather_far(j, back).wait_recv()
        for away in range(1, self.near):
            self.gather_near(j, away).start()

    def run(self, finish):
        def step(t, carry):
            for lag in range(self.bits + 1):
                j = t - lag

                @pl.when(jnp.logical_and(j >= 0, j < self.chunks))
                def _(lag=lag, j=j):
                    if lag < self.bits:
                        self.reduce(j, lag + 1, finish)
                    else:
                        self.relay(j)

            return carry

        lax.fori_loop(0, self.chunks + self.bits, step, 0)

    def consume(self, total, weight, weight_wait):
        full = self.refs.full
        rows, width = full.shape[3:]
        total[...] = jnp.zeros_like(total)

        def step(j, carry):
            weight_wait(j)
            for away in range(1, self.near):
                self.gather_near(j, away).wait_recv()
            product = jnp.dot(
                full[j].reshape(self.near * self.far * rows, width),
                weight[j],
                preferred_element_type=jnp.float32,
            )
            for block in range(self.near * self.far):
                place = block % self.near * self.far + block // self.near
                total[block * rows : (block + 1) * rows] += product[
                    place * rows : (place + 1) * rows
                ]
            return carry

        lax.fori_loop(0, self.chunks, step, 0)

    def drain(self):
        def step(j, carry):
            for away in range(1, self.near):
                self.gather_near(j, away).wait_send()
            for away in range(1, self.far):
                self.gather_far(j, away).wait_send()
            for k in range(self.bits):
                self.scatter(j, k).wait_send()
            return carry

        lax.fori_loop(0, self.chunks, step, 0)


def total_over_tp(refs, total, base, out, scale, tp, n_tp):
    part, slot, sems = refs.tp_part, refs.tp_slot, refs.tp_sem
    pieces, rows = part.shape[1], part.shape[3]
    half = total.shape[0] // 2
    core = bit(tp, 0)
    other = tp + 1 - 2 * core
    last = log2(n_tp)
    copies = []

    def send(src, dst, place, piece, peer):
        copy = to_tp(src, dst, sems.at[0, place, piece], sems.at[1, place, piece], peer)
        copy.start()
        copies.append(copy)
        return copy

    def window(piece):
        return pl.ds(piece * rows, rows)

    flying = []
    for piece in range(pieces):
        for side in range(2):
            start = side * half + piece * rows
            part[0, piece, side] = total[start : start + rows].astype(part.dtype)
        flying.append(
            send(part.at[0, piece, 1 - core], slot.at[0, piece], 0, piece, other)
        )
    for place in range(1, last + 1):
        for piece in range(pieces):
            flying[piece].wait_recv()
            own = part[0, piece, core] if place == 1 else part[place - 1, piece, 0]
            value = own.astype(jnp.float32) + slot[place - 1, piece].astype(jnp.float32)
            if place < last:
                part[place, piece, 0] = value.astype(part.dtype)
                peer = tp + (1 - 2 * bit(tp, place)) * (1 << place)
                flying[piece] = send(
                    part.at[place, piece, 0], slot.at[place, piece], place, piece, peer
                )
            else:
                kept = base[core, window(piece)].astype(jnp.float32)
                out[core, window(piece)] = (kept + scale * value).astype(out.dtype)
                rows_out = out.at[core, window(piece)]
                flying[piece] = send(rows_out, rows_out, last, piece, other)
    for copy in flying:
        copy.wait_recv()
    return copies


def exchange_scratch(n, chunks, rows, cols, width, row_shape):
    near, far = groups(n)
    shapes = SimpleNamespace()
    shapes.part = [
        pltpu.VMEM((chunks, 2, rows >> (k + 1), cols), jnp.bfloat16) for k in range(log2(n))
    ]
    shapes.slot = [
        pltpu.VMEM((chunks, rows >> (k + 1), cols), jnp.bfloat16) for k in range(log2(n))
    ]
    shapes.full = pltpu.VMEM((chunks, near, far, rows // n, width), jnp.bfloat16)
    shapes.scatter_sem = pltpu.SemaphoreType.DMA((2, log2(n), chunks))
    shapes.back_sem = pltpu.SemaphoreType.DMA((2, far - 1, chunks))
    shapes.relay_sem = pltpu.SemaphoreType.DMA((2, near - 1, chunks))
    shapes.row_part = pltpu.VMEM((n,) + row_shape, jnp.float32)
    shapes.row_slot = pltpu.VMEM((n - 1,) + row_shape, jnp.float32)
    shapes.row_sem = pltpu.SemaphoreType.DMA((2, n - 1))
    return shapes


def tp_scratch(n_tp, rows, cols):
    bits = log2(n_tp)
    return dict(
        tp_part=pltpu.VMEM((bits, PIECES, 2, rows // 2 // PIECES, cols), jnp.bfloat16),
        tp_slot=pltpu.VMEM((bits, PIECES, rows // 2 // PIECES, cols), jnp.bfloat16),
        tp_sem=pltpu.SemaphoreType.DMA((2, bits + 1, PIECES)),
    )


def chunks_of(columns):
    tiles = columns // LANES
    return max(d for d in range(1, 13) if tiles % d == 0)


def diagonal(size):
    rows = lax.broadcasted_iota(jnp.int32, (size, size), 0)
    return rows == lax.broadcasted_iota(jnp.int32, (size, size), 1)


def turn(values, axis):
    size = max(values.shape)
    spread = jnp.broadcast_to(values, (size, size))
    return jnp.sum(jnp.where(diagonal(size), spread, 0.0), axis=axis, keepdims=True)


def scale_rows(x, gain, scaled, kv):
    half, cols = x.shape[1:]
    columns = gain[:, pl.ds(pl.multiple_of(kv * cols, LANES), cols)]
    squares = []
    for side in range(2):
        values = x[side].astype(jnp.float32)
        squares.append(jnp.sum(values * values, axis=1, keepdims=True))
        scaled[side * half : (side + 1) * half] = (values * columns).astype(jnp.bfloat16)
    return jnp.concatenate(squares, axis=0)


class Feed:
    def __init__(self, refs, sources, kv, tp):
        self.refs, self.sources, self.kv, self.tp = refs, sources, kv, tp
        self.n, self.n_tp = lax.axis_size(KV), lax.axis_size(TP)
        self.chunks, self.width = refs.down.shape[:2]

    def fetch(self, j, side):
        columns = pl.ds(pl.multiple_of(j * self.width, LANES), self.width)
        return pltpu.make_async_copy(
            self.sources[side].at[:, columns],
            self.refs.weights.at[j, :, pl.ds(side * self.width, self.width)],
            self.refs.weight_sem.at[side, j],
        )

    def fetch_down(self, j):
        return pltpu.make_async_copy(
            self.sources[2].at[pl.ds(pl.multiple_of(j * self.width, LANES), self.width)],
            self.refs.down.at[j],
            self.refs.weight_sem.at[2, j],
        )

    def start_weights(self):
        def step(j, carry):
            self.fetch(j, 0).start()
            self.fetch(j, 1).start()
            return carry

        lax.fori_loop(0, self.chunks, step, 0)

    def start_down(self):
        def step(j, carry):
            self.fetch_down(j).start()
            return carry

        lax.fori_loop(0, self.chunks, step, 0)

    def run(self, x, gain, model_width):
        refs, kv, n, width = self.refs, self.kv, self.n, self.width
        squares = scale_rows(x, gain, refs.scaled, kv)
        rows = squares.shape[0]
        block = rows // n
        for peer in range(n):
            row = turn(squares[peer * block : (peer + 1) * block], 0)
            refs.row_part[peer, :, :block] = jnp.broadcast_to(row, (8, block))
        row_copies = sum_rows_start(refs, kv, n)
        exchange = Exchange(refs, kv, n, self.chunks)

        def product(j):
            self.fetch(j, 0).wait()
            self.fetch(j, 1).wait()
            return jnp.dot(
                refs.scaled[...], refs.weights[j], preferred_element_type=jnp.float32
            )

        exchange.produce(product)
        totals = sum_rows_finish(refs, row_copies, kv, n)
        row_scale = lax.rsqrt(turn(totals[:1, :block], 1) / model_width + EPSILON)
        refs.row_scale[...] = jnp.broadcast_to(row_scale, (block, LANES))

        def finish(j, sums):
            row_scale = refs.row_scale[:, :1]
            gate = row_scale * sums[:, :width]
            up = row_scale * sums[:, width:]
            return (jax.nn.silu(gate) * up).astype(jnp.bfloat16)

        exchange.run(finish)
        exchange.consume(refs.total, refs.down, lambda j: self.fetch_down(j).wait())

        def drain():
            exchange.drain()
            for copy in row_copies:
                copy.wait_send()

        return drain


def own_columns(refs, total, base, out, tp, n_tp):
    part, slot, sems = refs.out_part, refs.out_slot, refs.out_sem
    rows, own = part.shape[1:]
    half = rows // 2
    for piece in range(n_tp):
        part[piece] = total[:, piece * own : (piece + 1) * own].astype(part.dtype)
    copies = []
    for away in range(1, n_tp):
        peer = lax.rem(tp + away, n_tp)
        copy = to_tp(
            part.at[peer], slot.at[away - 1], sems.at[0, away - 1], sems.at[1, away - 1], peer
        )
        copy.start()
        copies.append(copy)
    value = part[tp].astype(jnp.float32)
    for away in range(1, n_tp):
        copies[away - 1].wait_recv()
        value = value + slot[away - 1].astype(jnp.float32)
    columns = pl.ds(pl.multiple_of(tp * own, LANES), own)
    for side in range(2):
        mine = base[side, :, columns].astype(jnp.float32)
        window = slice(side * half, (side + 1) * half)
        out[window] = (mine + 0.5 * value[window]).astype(out.dtype)
    return copies


class Mixer:
    def __init__(self, refs, io, kv, tp):
        self.refs, self.io, self.kv, self.tp = refs, io, kv, tp
        self.n, self.n_tp = lax.axis_size(KV), lax.axis_size(TP)
        self.heads, self.head_size, self.block_cols = refs.mix_out.shape
        self.slots = refs.state.shape[0]
        self.projections = (io.w_query, io.w_key, io.w_value, io.w_gate)

    def fetch(self, j, side):
        size = self.head_size
        return pltpu.make_async_copy(
            self.projections[side].at[:, pl.ds(pl.multiple_of(j * size, LANES), size)],
            self.refs.weights.at[j, :, pl.ds(side * size, size)],
            self.refs.weight_sem.at[side, j],
        )

    def fetch_mix(self, j):
        size = self.head_size
        return pltpu.make_async_copy(
            self.io.w_mix.at[pl.ds(pl.multiple_of(j * size, LANES), size)],
            self.refs.mix_out.at[j],
            self.refs.weight_sem.at[4, j],
        )

    def fetch_state(self, j):
        return pltpu.make_async_copy(
            self.io.previous.at[:, j],
            self.refs.state.at[lax.rem(j, self.slots)],
            self.refs.state_sem.at[j],
        )

    def fetch_small(self, side):
        start = pl.multiple_of(self.kv * self.block_cols, LANES)
        source = (self.io.w_beta, self.io.w_decay)[side]
        return pltpu.make_async_copy(
            source.at[:, pl.ds(start, self.block_cols)],
            self.refs.small_weights.at[side],
            self.refs.small_sem.at[side],
        )

    def start_fetches(self):
        self.fetch_small(0).start()
        self.fetch_small(1).start()

        def weights(j, carry):
            for side in range(4):
                self.fetch(j, side).start()
            self.fetch_mix(j).start()
            return carry

        def states(j, carry):
            self.fetch_state(j).start()
            return carry

        lax.fori_loop(0, self.heads, weights, 0)
        lax.fori_loop(0, self.slots, states, 0)

    def gates(self, totals, model_width):
        refs, io, heads = self.refs, self.io, self.heads
        all_heads = refs.small_weights.shape[1]
        block = totals.shape[0]
        row_scale = lax.rsqrt(
            totals[:, 2 * all_heads : 2 * all_heads + 1] / model_width + EPSILON
        )
        refs.row_scale[...] = jnp.broadcast_to(row_scale, (block, LANES))
        scaled_small = row_scale * totals
        lane = lax.broadcasted_iota(jnp.int32, (block, LANES), 1)
        span = jnp.floor(turn(io.lengths[...].astype(jnp.float32), 1) * (1.0 / SPAN))
        spans = io.span_bias.shape[1]
        matches = (
            lax.broadcasted_iota(jnp.int32, (block, spans), 1).astype(jnp.float32) == span
        )
        for h in range(heads):
            at = self.tp * heads + h
            beta_raw = jnp.sum(jnp.where(lane == at, scaled_small, 0.0), axis=1, keepdims=True)
            decay_raw = jnp.sum(
                jnp.where(lane == all_heads + at, scaled_small, 0.0), axis=1, keepdims=True
            )
            bias = jnp.sum(
                jnp.where(matches, io.span_bias[h : h + 1, :], 0.0), axis=1, keepdims=True
            )
            inner = decay_raw + io.decay_bias[:, h : h + 1] + bias
            soft = jnp.maximum(inner, 0.0) + jnp.log1p(jnp.exp(-jnp.abs(inner)))
            rate = jnp.exp(io.decay_rate[:, h : h + 1])
            decay = jnp.exp(-rate * soft + turn(io.extra[h : h + 1, :], 1))
            refs.decay[h] = jnp.broadcast_to(decay, (block, LANES))
            refs.beta[h] = jnp.broadcast_to(jax.nn.sigmoid(beta_raw), (block, LANES))

    def finish(self, j, sums):
        refs, io, size = self.refs, self.io, self.head_size
        block = sums.shape[0]

        def unit(raw):
            return raw * lax.rsqrt(jnp.sum(raw * raw, axis=1, keepdims=True) + EPSILON)

        sums = refs.row_scale[:, :1] * sums
        query = unit(jax.nn.silu(sums[:, :size])) * size ** (-0.5)
        key = unit(jax.nn.silu(sums[:, size : 2 * size]))
        value = jax.nn.silu(sums[:, 2 * size : 3 * size])
        gate = jax.nn.silu(sums[:, 3 * size :])
        refs.key[...] = key
        refs.value[...] = value
        refs.match[...] = jnp.broadcast_to(
            jnp.sum(key * query, axis=1, keepdims=True), (block, size)
        )
        refs.turned[...] = jnp.concatenate([key, query, value, gate], axis=0).T
        self.fetch_state(j).wait()
        slot = lax.rem(j, self.slots)
        for b in range(block):
            held = refs.state[slot, b]
            by_key = jnp.sum(held * refs.turned[:, b : b + 1], axis=0, keepdims=True)
            by_query = jnp.sum(
                held * refs.turned[:, block + b : block + b + 1], axis=0, keepdims=True
            )
            row = slice(b, b + 1)
            decay = refs.decay[j, row]
            write = refs.beta[j, row] * (refs.value[row] - decay * by_key)
            refs.readout[row] = decay * by_query + refs.match[row] * write
            io.decays[b, pl.ds(j, 1)] = decay
            io.keys[b, pl.ds(j, 1)] = refs.key[row]
            io.writes[b, pl.ds(j, 1)] = write

        @pl.when(j + self.slots < self.heads)
        def _():
            self.fetch_state(j + self.slots).start()

        readout = refs.readout[...]
        readout = (
            readout
            * lax.rsqrt(jnp.mean(readout * readout, axis=1, keepdims=True) + EPSILON)
            * io.head_gain[...]
            * gate
        )
        return readout.astype(jnp.bfloat16)

    def run(self, x, gain, model_width):
        refs, kv, n = self.refs, self.kv, self.n
        squares = scale_rows(x, gain, refs.scaled, kv)
        all_heads = refs.small_weights.shape[1]
        rows = squares.shape[0]
        small = refs.small
        small[...] = jnp.broadcast_to(squares, small.shape)
        for side in range(2):
            self.fetch_small(side).wait()
            small[:, side * all_heads : (side + 1) * all_heads] = lax.dot_general(
                refs.scaled[...],
                refs.small_weights[side],
                (((1,), (1,)), ((), ())),
                preferred_element_type=jnp.float32,
            )
        refs.row_part[...] = small[...].reshape(n, rows // n, LANES)
        row_copies = sum_rows_start(refs, kv, n)
        exchange = Exchange(refs, kv, n, self.heads)

        def product(j):
            for side in range(4):
                self.fetch(j, side).wait()
            return jnp.dot(
                refs.scaled[...], refs.weights[j], preferred_element_type=jnp.float32
            )

        exchange.produce(product)
        self.gates(sum_rows_finish(refs, row_copies, kv, n), model_width)
        exchange.run(self.finish)
        exchange.consume(refs.total, refs.mix_out, lambda j: self.fetch_mix(j).wait())

        def drain():
            exchange.drain()
            for copy in row_copies:
                copy.wait_send()

        return drain


def layer_kernel(model_width, aligned, io, refs):
    kv, tp = lax.axis_index(KV), lax.axis_index(TP)
    n, n_tp = lax.axis_size(KV), lax.axis_size(TP)
    feed, mix, blocks = refs.feed, refs.mix, refs.blocks
    half = blocks.shape[2]
    small_copies = []
    for item, (name, near) in enumerate(vars(refs.small).items()):
        copy = pltpu.make_async_copy(getattr(io, name), near, refs.small_sem.at[item])
        copy.start()
        small_copies.append(copy)
        setattr(io, name, near)
    if aligned:
        x_copies = [pltpu.make_async_copy(io.x, refs.pieces.at[tp], refs.x_sem.at[0])]
    else:
        x_copies = [
            pltpu.make_async_copy(
                io.x.at[pl.ds(side * half, half)], blocks.at[0, side], refs.x_sem.at[side]
            )
            for side in range(2)
        ]
    for copy in x_copies:
        copy.start()
    first = Feed(feed, (io.w_gate_one, io.w_up_one, io.w_down_one), kv, tp)
    second = Feed(feed, (io.w_gate_two, io.w_up_two, io.w_down_two), kv, tp)
    mixer = Mixer(mix, io, kv, tp)
    first.start_weights()
    meet(kv, tp, n, n_tp)
    for copy in x_copies:
        copy.wait()
    copies = []
    if aligned:
        own = io.x.shape[1]
        for away in range(1, n_tp):
            copy = to_tp(
                refs.pieces.at[tp],
                refs.pieces.at[tp],
                refs.piece_sem.at[0, away - 1],
                refs.piece_sem.at[1, away - 1],
                lax.rem(tp + away, n_tp),
            )
            copy.start()
            copies.append(copy)
    first.start_down()
    mixer.start_fetches()
    for copy in small_copies:
        copy.wait()
    for copy in copies:
        copy.wait_recv()
    if aligned:
        for piece in range(n_tp):
            columns = slice(piece * own, (piece + 1) * own)
            blocks[0, 0, :, columns] = refs.pieces[piece, :half]
            blocks[0, 1, :, columns] = refs.pieces[piece, half:]
    drain = first.run(blocks.at[0], io.gain_one, model_width)
    second.start_weights()
    second.start_down()
    copies += total_over_tp(
        refs.sums_one, feed.total, blocks.at[0], blocks.at[1], 0.5, tp, n_tp
    )
    drain_mixer = mixer.run(blocks.at[1], io.gain_mix, model_width)
    drain()
    copies += total_over_tp(refs.sums_mix, mix.total, blocks.at[1], blocks.at[2], 1.0, tp, n_tp)
    drain = second.run(blocks.at[2], io.gain_two, model_width)
    if aligned:
        copies += own_columns(refs, feed.total, blocks.at[2], io.out, tp, n_tp)
    else:
        copies += total_over_tp(refs.sums_two, feed.total, blocks.at[2], io.out, 0.5, tp, n_tp)
    drain()
    drain_mixer()
    for copy in copies:
        copy.wait_send()


def spaced(tree):
    if isinstance(tree, dict):
        return SimpleNamespace(**{name: spaced(leaf) for name, leaf in tree.items()})
    return tree


def call_kernel(kernel, inputs, outputs, scratch, name, call_id):
    arrays = [array for array, _ in inputs.values()]
    leaves, tree = jax.tree.flatten(scratch)

    def entry(*given):
        io = dict(zip([*inputs, *outputs], given))
        kernel(spaced(io), spaced(jax.tree.unflatten(tree, given[len(io) :])))

    return pl.pallas_call(
        entry,
        out_shape=[shape for shape, _ in outputs.values()],
        in_specs=[pl.BlockSpec(memory_space=space) for _, space in inputs.values()],
        out_specs=[pl.BlockSpec(memory_space=space) for _, space in outputs.values()],
        scratch_shapes=leaves,
        name=name,
        compiler_params=pltpu.CompilerParams(
            collective_id=call_id, has_side_effects=True, vmem_limit_bytes=LIMIT
        ),
    )(*arrays)


def row_scratch(scratch, rows, block_cols, n):
    scratch.scaled = pltpu.VMEM((rows, block_cols), jnp.bfloat16)
    scratch.row_scale = pltpu.VMEM((rows // n, LANES), jnp.float32)
    scratch.total = pltpu.VMEM((rows, block_cols), jnp.float32)
    return vars(scratch)


def layer(
    x,
    previous_state,
    lengths,
    gain_one,
    w_gate_one,
    w_up_one,
    w_down_one,
    gain_mix,
    w_query,
    w_key,
    w_value,
    w_gate,
    w_beta,
    w_decay,
    decay_rate,
    decay_bias,
    span_bias,
    extra,
    head_gain,
    w_mix,
    gain_two,
    w_gate_two,
    w_up_two,
    w_down_two,
    aligned,
):
    n, n_tp = lax.axis_size(KV), lax.axis_size(TP)
    rows = x.shape[0]
    block_cols, columns = w_gate_one.shape
    own = block_cols // n_tp
    block, heads, head_size = previous_state.shape[:3]
    all_heads = w_beta.shape[1]
    chunks = chunks_of(columns)
    width = columns // chunks
    vmem, hbm = pltpu.VMEM, pltpu.HBM

    def far(array):
        return (pltpu.with_memory_space_constraint(array, hbm), hbm)

    def row(array):
        return array.reshape(1, -1)

    small = dict(
        gain_one=row(gain_one),
        gain_mix=row(gain_mix),
        gain_two=row(gain_two),
        lengths=row(lengths),
        span_bias=span_bias,
        extra=extra.T,
        head_gain=row(head_gain),
        decay_rate=row(decay_rate),
        decay_bias=row(decay_bias),
    )
    inputs = dict(
        x=far(x),
        w_gate_one=far(w_gate_one),
        w_up_one=far(w_up_one),
        w_down_one=far(w_down_one),
        w_query=far(w_query),
        w_key=far(w_key),
        w_value=far(w_value),
        w_gate=far(w_gate),
        w_beta=far(w_beta.T),
        w_decay=far(w_decay.T),
        w_mix=far(w_mix),
        w_gate_two=far(w_gate_two),
        w_up_two=far(w_up_two),
        w_down_two=far(w_down_two),
        previous=far(previous_state),
        **{name: far(array) for name, array in small.items()},
    )
    shape = (rows, own) if aligned else (2, rows // 2, block_cols)
    rows_of_heads = jax.ShapeDtypeStruct((block, heads, head_size), jnp.float32)
    outputs = dict(
        out=(jax.ShapeDtypeStruct(shape, jnp.bfloat16), vmem),
        decays=(rows_of_heads, vmem),
        keys=(rows_of_heads, vmem),
        writes=(rows_of_heads, vmem),
    )
    feed = exchange_scratch(n, chunks, rows, 2 * width, width, (8, LANES))
    feed.weights = vmem((chunks, block_cols, 2 * width), jnp.bfloat16)
    feed.down = vmem((chunks, width, block_cols), jnp.bfloat16)
    feed.weight_sem = pltpu.SemaphoreType.DMA((3, chunks))
    mix = exchange_scratch(n, heads, rows, 4 * head_size, head_size, (block, LANES))
    mix.weights = vmem((heads, block_cols, 4 * head_size), jnp.bfloat16)
    mix.mix_out = vmem((heads, head_size, block_cols), jnp.bfloat16)
    mix.weight_sem = pltpu.SemaphoreType.DMA((5, heads))
    mix.state = vmem((min(heads, 4), block, head_size, head_size), jnp.float32)
    mix.state_sem = pltpu.SemaphoreType.DMA((heads,))
    mix.small_weights = vmem((2, all_heads, block_cols), jnp.bfloat16)
    mix.small_sem = pltpu.SemaphoreType.DMA((2,))
    mix.small = vmem((rows, LANES), jnp.float32)
    mix.decay = vmem((heads, block, LANES), jnp.float32)
    mix.beta = vmem((heads, block, LANES), jnp.float32)
    mix.key = vmem((block, head_size), jnp.float32)
    mix.value = vmem((block, head_size), jnp.float32)
    mix.match = vmem((block, head_size), jnp.float32)
    mix.readout = vmem((block, head_size), jnp.float32)
    mix.turned = vmem((head_size, 4 * block), jnp.float32)
    scratch = dict(
        feed=row_scratch(feed, rows, block_cols, n),
        mix=row_scratch(mix, rows, block_cols, n),
        blocks=vmem((3, 2, rows // 2, block_cols), jnp.bfloat16),
        sums_one=tp_scratch(n_tp, rows, block_cols),
        sums_mix=tp_scratch(n_tp, rows, block_cols),
        small={name: vmem(array.shape, array.dtype) for name, array in small.items()},
        small_sem=pltpu.SemaphoreType.DMA((len(small),)),
        x_sem=pltpu.SemaphoreType.DMA((2,)),
    )
    if aligned:
        scratch.update(
            pieces=vmem((n_tp, rows, own), jnp.bfloat16),
            piece_sem=pltpu.SemaphoreType.DMA((2, n_tp - 1)),
            out_part=vmem((n_tp, rows, own), jnp.bfloat16),
            out_slot=vmem((n_tp - 1, rows, own), jnp.bfloat16),
            out_sem=pltpu.SemaphoreType.DMA((2, n_tp - 1)),
        )
    else:
        scratch.update(sums_two=tp_scratch(n_tp, rows, block_cols))
    out, decays, keys, writes = call_kernel(
        functools.partial(layer_kernel, gain_one.shape[0], aligned),
        inputs,
        outputs,
        scratch,
        "layer",
        0,
    )
    return out if aligned else out.reshape(rows, block_cols), decays, keys, writes


def body(
    tokens,
    previous_state,
    lengths,
    first_feed_norm_gain,
    first_gate_projection,
    first_up_projection,
    first_down_projection,
    mixer_norm_gain,
    query_weight,
    key_weight,
    value_weight,
    output_gate_weight,
    write_strength_weight,
    decay_input_weight,
    head_log_decay_rate,
    decay_input_bias,
    length_span_bias,
    extra_log_decay,
    readout_head_norm_gain,
    mixer_output_weight,
    second_feed_norm_gain,
    second_gate_projection,
    second_up_projection,
    second_down_projection,
):
    own_cols = tokens.shape[1]
    aligned = own_cols % LANES == 0
    if not aligned:
        tokens = lax.all_gather(tokens, TP, axis=1, tiled=True)
    result, decays, keys, writes = layer(
        tokens,
        previous_state,
        lengths,
        first_feed_norm_gain,
        first_gate_projection,
        first_up_projection,
        first_down_projection,
        mixer_norm_gain,
        query_weight,
        key_weight,
        value_weight,
        output_gate_weight,
        write_strength_weight,
        decay_input_weight,
        head_log_decay_rate,
        decay_input_bias,
        length_span_bias,
        extra_log_decay,
        readout_head_norm_gain,
        mixer_output_weight,
        second_feed_norm_gain,
        second_gate_projection,
        second_up_projection,
        second_down_projection,
        aligned,
    )
    new_state = (
        decays[:, :, None, :] * previous_state + keys[:, :, :, None] * writes[:, :, None, :]
    )
    if not aligned:
        start = lax.axis_index(TP) * own_cols
        result = lax.dynamic_slice_in_dim(result, start, own_cols, 1)
    return (result, new_state)


def solution(mesh):
    return jax.shard_map(
        body,
        mesh=mesh,
        in_specs=(
            P(None, (KV, TP)),
            P(KV, TP, None, None),
            P(KV),
            P(),
            P(KV, TP),
            P(KV, TP),
            P(TP, KV),
            P(),
            P(KV, TP),
            P(KV, TP),
            P(KV, TP),
            P(KV, TP),
            P(),
            P(),
            P(TP),
            P(TP),
            P(TP, None),
            P(KV, TP),
            P(),
            P(TP, KV),
            P(),
            P(KV, TP),
            P(KV, TP),
            P(TP, KV),
        ),
        out_specs=(P(None, (KV, TP)), P(KV, TP, None, None)),
        check_vma=False,
    )
```

```python
import functools
from types import SimpleNamespace

import jax
import jax.numpy as jnp
from jax import lax
from jax.experimental import pallas as pl
from jax.experimental.pallas import tpu as pltpu
from jax.sharding import PartitionSpec as P

SPAN = 1024


EPSILON = 1e-06


LANES = 128


LIMIT = 46 << 20


PIECES = 2


SKEW = 2


KV = "kv"


TP = "tp"


MESH = pl.DeviceIdType.MESH


def log2(n):
    return n.bit_length() - 1


def bit(value, place):
    return lax.rem(value // (1 << place), 2)


def place_of(block, bits):
    return sum(((block >> k) & 1) << (bits - 1 - k) for k in range(bits))


def groups(n):
    near = max(n // 4, 2)
    return near, n // near


def meet(kv, tp, n_kv, n_tp):
    barrier = pltpu.get_barrier_semaphore()
    for away in range(1, n_kv):
        pl.semaphore_signal(
            barrier, inc=1, device_id={KV: lax.rem(kv + away, n_kv)}, device_id_type=MESH
        )
    for away in range(1, n_tp):
        pl.semaphore_signal(
            barrier, inc=1, device_id={TP: lax.rem(tp + away, n_tp)}, device_id_type=MESH
        )
    pl.semaphore_wait(barrier, n_kv + n_tp - 2)


def to_kv(src, dst, send, recv, peer):
    return pltpu.make_async_remote_copy(
        src_ref=src,
        dst_ref=dst,
        send_sem=send,
        recv_sem=recv,
        device_id={KV: peer},
        device_id_type=MESH,
    )


def to_tp(src, dst, send, recv, peer):
    return pltpu.make_async_remote_copy(
        src_ref=src,
        dst_ref=dst,
        send_sem=send,
        recv_sem=recv,
        device_id={TP: peer},
        device_id_type=MESH,
    )


def sum_rows_start(refs, kv, n):
    copies = []
    for away in range(1, n):
        peer = lax.rem(kv + away, n)
        copy = to_kv(
            refs.row_part.at[peer],
            refs.row_slot.at[away - 1],
            refs.row_sem.at[0, away - 1],
            refs.row_sem.at[1, away - 1],
            peer,
        )
        copy.start()
        copies.append(copy)
    return copies


def sum_rows_finish(refs, copies, kv, n):
    for copy in copies:
        copy.wait_recv()
    total = refs.row_part[kv]
    for away in range(n - 1):
        total = total + refs.row_slot[away]
    return total


class Exchange:
    def __init__(self, refs, kv, n, chunks):
        self.refs, self.chunks, self.kv, self.n = refs, chunks, kv, n
        self.bits = log2(n)
        self.near, self.far = groups(n)
        self.outer, self.inner = kv // self.near, lax.rem(kv, self.near)

    def inner_peer(self, away):
        return lax.rem(self.inner + away, self.near)

    def outer_peer(self, away):
        return sum(
            lax.rem(bit(self.outer, k) + (away >> k), 2) * (1 << k)
            for k in range(log2(self.far))
        )

    def scatter(self, j, k):
        side = bit(self.kv, k)
        return to_kv(
            self.refs.part[k].at[j, 1 - side],
            self.refs.slot[k].at[j],
            self.refs.scatter_sem.at[0, k, j],
            self.refs.scatter_sem.at[1, k, j],
            self.kv + (1 - 2 * side) * (1 << k),
        )

    def gather_far(self, j, away):
        own = self.refs.full.at[j, self.inner, self.outer]
        return to_kv(
            own,
            own,
            self.refs.back_sem.at[0, away - 1, j],
            self.refs.back_sem.at[1, away - 1, j],
            self.outer_peer(away) * self.near + self.inner,
        )

    def gather_near(self, j, away):
        window = self.refs.full.at[j, self.inner]
        return to_kv(
            window,
            window,
            self.refs.relay_sem.at[0, away - 1, j],
            self.refs.relay_sem.at[1, away - 1, j],
            self.outer * self.near + self.inner_peer(away),
        )

    def produce(self, product):
        part = self.refs.part[0]
        rows = self.refs.slot[-1].shape[1]
        half = self.n // 2

        def step(j, carry):
            value = product(j)
            for block in range(self.n):
                place = place_of(block, self.bits)
                start = place % half * rows
                part[j, place // half, start : start + rows] = value[
                    block * rows : (block + 1) * rows
                ].astype(part.dtype)
            self.scatter(j, 0).start()
            return carry

        lax.fori_loop(0, self.chunks, step, 0)

    def reduce(self, j, k, finish):
        self.scatter(j, k - 1).wait_recv()
        total = self.refs.part[k - 1][j, bit(self.kv, k - 1)].astype(jnp.float32)
        total = total + self.refs.slot[k - 1][j].astype(jnp.float32)
        if k < self.bits:
            part = self.refs.part[k]
            rows = total.shape[0] // 2
            part[j, 0] = total[:rows].astype(part.dtype)
            part[j, 1] = total[rows:].astype(part.dtype)
            self.scatter(j, k).start()
            return
        self.refs.full[j, self.inner, self.outer] = finish(j, total)
        for away in range(1, self.far):
            self.gather_far(j, away).start()

    def relay(self, j):
        for back in range(1, self.far):
            self.gather_far(j, back).wait_recv()
        for away in range(1, self.near):
            self.gather_near(j, away).start()

    def run(self, finish):
        def step(t, carry):
            for lag in range(self.bits + 1):
                j = t - SKEW * lag

                @pl.when(jnp.logical_and(j >= 0, j < self.chunks))
                def _(lag=lag, j=j):
                    if lag < self.bits:
                        self.reduce(j, lag + 1, finish)
                    else:
                        self.relay(j)

            return carry

        lax.fori_loop(0, self.chunks + SKEW * self.bits, step, 0)

    def consume(self, total, weight, weight_wait):
        full = self.refs.full
        rows, width = full.shape[3:]
        total[...] = jnp.zeros_like(total)

        def step(j, carry):
            weight_wait(j)
            for away in range(1, self.near):
                self.gather_near(j, away).wait_recv()
            product = jnp.dot(
                full[j].reshape(self.near * self.far * rows, width),
                weight[j],
                preferred_element_type=jnp.float32,
            )
            for block in range(self.near * self.far):
                place = block % self.near * self.far + block // self.near
                total[block * rows : (block + 1) * rows] += product[
                    place * rows : (place + 1) * rows
                ]
            return carry

        lax.fori_loop(0, self.chunks, step, 0)

    def drain(self):
        def step(j, carry):
            for away in range(1, self.near):
                self.gather_near(j, away).wait_send()
            for away in range(1, self.far):
                self.gather_far(j, away).wait_send()
            for k in range(self.bits):
                self.scatter(j, k).wait_send()
            return carry

        lax.fori_loop(0, self.chunks, step, 0)


def total_over_tp(refs, total, base, out, scale, tp, n_tp):
    part, slot, sems = refs.tp_part, refs.tp_slot, refs.tp_sem
    pieces, rows = part.shape[1], part.shape[3]
    half = total.shape[0] // 2
    core = bit(tp, 0)
    other = tp + 1 - 2 * core
    last = log2(n_tp)
    copies = []

    def send(src, dst, place, piece, peer):
        copy = to_tp(src, dst, sems.at[0, place, piece], sems.at[1, place, piece], peer)
        copy.start()
        copies.append(copy)
        return copy

    def window(piece):
        return pl.ds(piece * rows, rows)

    flying = []
    for piece in range(pieces):
        for side in range(2):
            start = side * half + piece * rows
            part[0, piece, side] = total[start : start + rows].astype(part.dtype)
        flying.append(
            send(part.at[0, piece, 1 - core], slot.at[0, piece], 0, piece, other)
        )
    for place in range(1, last + 1):
        for piece in range(pieces):
            flying[piece].wait_recv()
            own = part[0, piece, core] if place == 1 else part[place - 1, piece, 0]
            value = own.astype(jnp.float32) + slot[place - 1, piece].astype(jnp.float32)
            if place < last:
                part[place, piece, 0] = value.astype(part.dtype)
                peer = tp + (1 - 2 * bit(tp, place)) * (1 << place)
                flying[piece] = send(
                    part.at[place, piece, 0], slot.at[place, piece], place, piece, peer
                )
            else:
                kept = base[core, window(piece)].astype(jnp.float32)
                out[core, window(piece)] = (kept + scale * value).astype(out.dtype)
                rows_out = out.at[core, window(piece)]
                flying[piece] = send(rows_out, rows_out, last, piece, other)
    for copy in flying:
        copy.wait_recv()
    return copies


def exchange_scratch(n, chunks, rows, cols, width, row_shape):
    near, far = groups(n)
    shapes = SimpleNamespace()
    shapes.part = [
        pltpu.VMEM((chunks, 2, rows >> (k + 1), cols), jnp.bfloat16) for k in range(log2(n))
    ]
    shapes.slot = [
        pltpu.VMEM((chunks, rows >> (k + 1), cols), jnp.bfloat16) for k in range(log2(n))
    ]
    shapes.full = pltpu.VMEM((chunks, near, far, rows // n, width), jnp.bfloat16)
    shapes.scatter_sem = pltpu.SemaphoreType.DMA((2, log2(n), chunks))
    shapes.back_sem = pltpu.SemaphoreType.DMA((2, far - 1, chunks))
    shapes.relay_sem = pltpu.SemaphoreType.DMA((2, near - 1, chunks))
    shapes.row_part = pltpu.VMEM((n,) + row_shape, jnp.float32)
    shapes.row_slot = pltpu.VMEM((n - 1,) + row_shape, jnp.float32)
    shapes.row_sem = pltpu.SemaphoreType.DMA((2, n - 1))
    return shapes


def tp_scratch(n_tp, rows, cols):
    bits = log2(n_tp)
    return dict(
        tp_part=pltpu.VMEM((bits, PIECES, 2, rows // 2 // PIECES, cols), jnp.bfloat16),
        tp_slot=pltpu.VMEM((bits, PIECES, rows // 2 // PIECES, cols), jnp.bfloat16),
        tp_sem=pltpu.SemaphoreType.DMA((2, bits + 1, PIECES)),
    )


def chunks_of(columns):
    tiles = columns // LANES
    return max(d for d in range(1, 13) if tiles % d == 0)


def diagonal(size):
    rows = lax.broadcasted_iota(jnp.int32, (size, size), 0)
    return rows == lax.broadcasted_iota(jnp.int32, (size, size), 1)


def turn(values, axis):
    size = max(values.shape)
    spread = jnp.broadcast_to(values, (size, size))
    return jnp.sum(jnp.where(diagonal(size), spread, 0.0), axis=axis, keepdims=True)


def scale_rows(x, gain, scaled, kv):
    half, cols = x.shape[1:]
    columns = gain[:, pl.ds(pl.multiple_of(kv * cols, LANES), cols)]
    squares = []
    for side in range(2):
        values = x[side].astype(jnp.float32)
        squares.append(jnp.sum(values * values, axis=1, keepdims=True))
        scaled[side * half : (side + 1) * half] = (values * columns).astype(jnp.bfloat16)
    return jnp.concatenate(squares, axis=0)


class Feed:
    def __init__(self, refs, sources, kv, tp):
        self.refs, self.sources, self.kv, self.tp = refs, sources, kv, tp
        self.n, self.n_tp = lax.axis_size(KV), lax.axis_size(TP)
        self.chunks, self.width = refs.down.shape[:2]

    def fetch(self, j, side):
        columns = pl.ds(pl.multiple_of(j * self.width, LANES), self.width)
        return pltpu.make_async_copy(
            self.sources[side].at[:, columns],
            self.refs.weights.at[j, :, pl.ds(side * self.width, self.width)],
            self.refs.weight_sem.at[side, j],
        )

    def fetch_down(self, j):
        return pltpu.make_async_copy(
            self.sources[2].at[pl.ds(pl.multiple_of(j * self.width, LANES), self.width)],
            self.refs.down.at[j],
            self.refs.weight_sem.at[2, j],
        )

    def start_weights(self):
        def step(j, carry):
            self.fetch(j, 0).start()
            self.fetch(j, 1).start()
            return carry

        lax.fori_loop(0, self.chunks, step, 0)

    def start_down(self):
        def step(j, carry):
            self.fetch_down(j).start()
            return carry

        lax.fori_loop(0, self.chunks, step, 0)

    def run(self, x, gain, model_width):
        refs, kv, n, width = self.refs, self.kv, self.n, self.width
        squares = scale_rows(x, gain, refs.scaled, kv)
        rows = squares.shape[0]
        block = rows // n
        for peer in range(n):
            row = turn(squares[peer * block : (peer + 1) * block], 0)
            refs.row_part[peer, :, :block] = jnp.broadcast_to(row, (8, block))
        row_copies = sum_rows_start(refs, kv, n)
        exchange = Exchange(refs, kv, n, self.chunks)

        def product(j):
            self.fetch(j, 0).wait()
            self.fetch(j, 1).wait()
            return jnp.dot(
                refs.scaled[...], refs.weights[j], preferred_element_type=jnp.float32
            )

        exchange.produce(product)
        totals = sum_rows_finish(refs, row_copies, kv, n)
        row_scale = lax.rsqrt(turn(totals[:1, :block], 1) / model_width + EPSILON)
        refs.row_scale[...] = jnp.broadcast_to(row_scale, (block, LANES))

        def finish(j, sums):
            row_scale = refs.row_scale[:, :1]
            gate = row_scale * sums[:, :width]
            up = row_scale * sums[:, width:]
            return (jax.nn.silu(gate) * up).astype(jnp.bfloat16)

        exchange.run(finish)
        exchange.consume(refs.total, refs.down, lambda j: self.fetch_down(j).wait())

        def drain():
            exchange.drain()
            for copy in row_copies:
                copy.wait_send()

        return drain


def own_columns(refs, total, base, out, tp, n_tp):
    part, slot, sems = refs.out_part, refs.out_slot, refs.out_sem
    rows, own = part.shape[1:]
    half = rows // 2
    for piece in range(n_tp):
        part[piece] = total[:, piece * own : (piece + 1) * own].astype(part.dtype)
    copies = []
    for away in range(1, n_tp):
        peer = lax.rem(tp + away, n_tp)
        copy = to_tp(
            part.at[peer], slot.at[away - 1], sems.at[0, away - 1], sems.at[1, away - 1], peer
        )
        copy.start()
        copies.append(copy)
    value = part[tp].astype(jnp.float32)
    for away in range(1, n_tp):
        copies[away - 1].wait_recv()
        value = value + slot[away - 1].astype(jnp.float32)
    columns = pl.ds(pl.multiple_of(tp * own, LANES), own)
    for side in range(2):
        mine = base[side, :, columns].astype(jnp.float32)
        window = slice(side * half, (side + 1) * half)
        out[window] = (mine + 0.5 * value[window]).astype(out.dtype)
    return copies


class Mixer:
    def __init__(self, refs, io, kv, tp):
        self.refs, self.io, self.kv, self.tp = refs, io, kv, tp
        self.n, self.n_tp = lax.axis_size(KV), lax.axis_size(TP)
        self.heads, self.head_size, self.block_cols = refs.mix_out.shape
        self.slots = refs.state.shape[0]
        self.projections = (io.w_query, io.w_key, io.w_value, io.w_gate)

    def fetch(self, j, side):
        size = self.head_size
        return pltpu.make_async_copy(
            self.projections[side].at[:, pl.ds(pl.multiple_of(j * size, LANES), size)],
            self.refs.weights.at[j, :, pl.ds(side * size, size)],
            self.refs.weight_sem.at[side, j],
        )

    def fetch_mix(self, j):
        size = self.head_size
        return pltpu.make_async_copy(
            self.io.w_mix.at[pl.ds(pl.multiple_of(j * size, LANES), size)],
            self.refs.mix_out.at[j],
            self.refs.weight_sem.at[4, j],
        )

    def fetch_state(self, j):
        return pltpu.make_async_copy(
            self.io.previous.at[:, j],
            self.refs.state.at[lax.rem(j, self.slots)],
            self.refs.state_sem.at[j],
        )

    def fetch_small(self, side):
        start = pl.multiple_of(self.kv * self.block_cols, LANES)
        source = (self.io.w_beta, self.io.w_decay)[side]
        return pltpu.make_async_copy(
            source.at[:, pl.ds(start, self.block_cols)],
            self.refs.small_weights.at[side],
            self.refs.small_sem.at[side],
        )

    def start_fetches(self):
        self.fetch_small(0).start()
        self.fetch_small(1).start()

        def weights(j, carry):
            for side in range(4):
                self.fetch(j, side).start()
            self.fetch_mix(j).start()
            return carry

        def states(j, carry):
            self.fetch_state(j).start()
            return carry

        lax.fori_loop(0, self.heads, weights, 0)
        lax.fori_loop(0, self.slots, states, 0)

    def gates(self, totals, model_width):
        refs, io, heads = self.refs, self.io, self.heads
        all_heads = refs.small_weights.shape[1]
        block = totals.shape[0]
        row_scale = lax.rsqrt(
            totals[:, 2 * all_heads : 2 * all_heads + 1] / model_width + EPSILON
        )
        refs.row_scale[...] = jnp.broadcast_to(row_scale, (block, LANES))
        scaled_small = row_scale * totals
        lane = lax.broadcasted_iota(jnp.int32, (block, LANES), 1)
        span = jnp.floor(turn(io.lengths[...].astype(jnp.float32), 1) * (1.0 / SPAN))
        spans = io.span_bias.shape[1]
        matches = (
            lax.broadcasted_iota(jnp.int32, (block, spans), 1).astype(jnp.float32) == span
        )
        for h in range(heads):
            at = self.tp * heads + h
            beta_raw = jnp.sum(jnp.where(lane == at, scaled_small, 0.0), axis=1, keepdims=True)
            decay_raw = jnp.sum(
                jnp.where(lane == all_heads + at, scaled_small, 0.0), axis=1, keepdims=True
            )
            bias = jnp.sum(
                jnp.where(matches, io.span_bias[h : h + 1, :], 0.0), axis=1, keepdims=True
            )
            inner = decay_raw + io.decay_bias[:, h : h + 1] + bias
            soft = jnp.maximum(inner, 0.0) + jnp.log1p(jnp.exp(-jnp.abs(inner)))
            rate = jnp.exp(io.decay_rate[:, h : h + 1])
            decay = jnp.exp(-rate * soft + turn(io.extra[h : h + 1, :], 1))
            refs.decay[h] = jnp.broadcast_to(decay, (block, LANES))
            refs.beta[h] = jnp.broadcast_to(jax.nn.sigmoid(beta_raw), (block, LANES))

    def finish(self, j, sums):
        refs, io, size = self.refs, self.io, self.head_size
        block = sums.shape[0]

        def unit(raw):
            return raw * lax.rsqrt(jnp.sum(raw * raw, axis=1, keepdims=True) + EPSILON)

        sums = refs.row_scale[:, :1] * sums
        query = unit(jax.nn.silu(sums[:, :size])) * size ** (-0.5)
        key = unit(jax.nn.silu(sums[:, size : 2 * size]))
        value = jax.nn.silu(sums[:, 2 * size : 3 * size])
        gate = jax.nn.silu(sums[:, 3 * size :])
        refs.key[...] = key
        refs.value[...] = value
        refs.match[...] = jnp.broadcast_to(
            jnp.sum(key * query, axis=1, keepdims=True), (block, size)
        )
        refs.turned[...] = jnp.concatenate([key, query, value, gate], axis=0).T
        self.fetch_state(j).wait()
        slot = lax.rem(j, self.slots)
        for b in range(block):
            held = refs.state[slot, b]
            by_key = jnp.sum(held * refs.turned[:, b : b + 1], axis=0, keepdims=True)
            by_query = jnp.sum(
                held * refs.turned[:, block + b : block + b + 1], axis=0, keepdims=True
            )
            row = slice(b, b + 1)
            decay = refs.decay[j, row]
            write = refs.beta[j, row] * (refs.value[row] - decay * by_key)
            refs.readout[row] = decay * by_query + refs.match[row] * write
            io.decays[b, pl.ds(j, 1)] = decay
            io.keys[b, pl.ds(j, 1)] = refs.key[row]
            io.writes[b, pl.ds(j, 1)] = write

        @pl.when(j + self.slots < self.heads)
        def _():
            self.fetch_state(j + self.slots).start()

        readout = refs.readout[...]
        readout = (
            readout
            * lax.rsqrt(jnp.mean(readout * readout, axis=1, keepdims=True) + EPSILON)
            * io.head_gain[...]
            * gate
        )
        return readout.astype(jnp.bfloat16)

    def run(self, x, gain, model_width):
        refs, kv, n = self.refs, self.kv, self.n
        squares = scale_rows(x, gain, refs.scaled, kv)
        all_heads = refs.small_weights.shape[1]
        rows = squares.shape[0]
        small = refs.small
        small[...] = jnp.broadcast_to(squares, small.shape)
        for side in range(2):
            self.fetch_small(side).wait()
            small[:, side * all_heads : (side + 1) * all_heads] = lax.dot_general(
                refs.scaled[...],
                refs.small_weights[side],
                (((1,), (1,)), ((), ())),
                preferred_element_type=jnp.float32,
            )
        refs.row_part[...] = small[...].reshape(n, rows // n, LANES)
        row_copies = sum_rows_start(refs, kv, n)
        exchange = Exchange(refs, kv, n, self.heads)

        def product(j):
            for side in range(4):
                self.fetch(j, side).wait()
            return jnp.dot(
                refs.scaled[...], refs.weights[j], preferred_element_type=jnp.float32
            )

        exchange.produce(product)
        self.gates(sum_rows_finish(refs, row_copies, kv, n), model_width)
        exchange.run(self.finish)
        exchange.consume(refs.total, refs.mix_out, lambda j: self.fetch_mix(j).wait())

        def drain():
            exchange.drain()
            for copy in row_copies:
                copy.wait_send()

        return drain


def layer_kernel(model_width, aligned, io, refs):
    kv, tp = lax.axis_index(KV), lax.axis_index(TP)
    n, n_tp = lax.axis_size(KV), lax.axis_size(TP)
    feed, mix, blocks = refs.feed, refs.mix, refs.blocks
    half = blocks.shape[2]
    small_copies = []
    for item, (name, near) in enumerate(vars(refs.small).items()):
        copy = pltpu.make_async_copy(getattr(io, name), near, refs.small_sem.at[item])
        copy.start()
        small_copies.append(copy)
        setattr(io, name, near)
    if aligned:
        x_copies = [pltpu.make_async_copy(io.x, refs.pieces.at[tp], refs.x_sem.at[0])]
    else:
        x_copies = [
            pltpu.make_async_copy(
                io.x.at[pl.ds(side * half, half)], blocks.at[0, side], refs.x_sem.at[side]
            )
            for side in range(2)
        ]
    for copy in x_copies:
        copy.start()
    first = Feed(feed, (io.w_gate_one, io.w_up_one, io.w_down_one), kv, tp)
    second = Feed(feed, (io.w_gate_two, io.w_up_two, io.w_down_two), kv, tp)
    mixer = Mixer(mix, io, kv, tp)
    first.start_weights()
    meet(kv, tp, n, n_tp)
    for copy in x_copies:
        copy.wait()
    copies = []
    if aligned:
        own = io.x.shape[1]
        for away in range(1, n_tp):
            copy = to_tp(
                refs.pieces.at[tp],
                refs.pieces.at[tp],
                refs.piece_sem.at[0, away - 1],
                refs.piece_sem.at[1, away - 1],
                lax.rem(tp + away, n_tp),
            )
            copy.start()
            copies.append(copy)
    first.start_down()
    mixer.start_fetches()
    for copy in small_copies:
        copy.wait()
    for copy in copies:
        copy.wait_recv()
    if aligned:
        for piece in range(n_tp):
            columns = slice(piece * own, (piece + 1) * own)
            blocks[0, 0, :, columns] = refs.pieces[piece, :half]
            blocks[0, 1, :, columns] = refs.pieces[piece, half:]
    drain = first.run(blocks.at[0], io.gain_one, model_width)
    second.start_weights()
    second.start_down()
    copies += total_over_tp(
        refs.sums_one, feed.total, blocks.at[0], blocks.at[1], 0.5, tp, n_tp
    )
    drain_mixer = mixer.run(blocks.at[1], io.gain_mix, model_width)
    drain()
    copies += total_over_tp(refs.sums_mix, mix.total, blocks.at[1], blocks.at[2], 1.0, tp, n_tp)
    drain = second.run(blocks.at[2], io.gain_two, model_width)
    if aligned:
        copies += own_columns(refs, feed.total, blocks.at[2], io.out, tp, n_tp)
    else:
        copies += total_over_tp(refs.sums_two, feed.total, blocks.at[2], io.out, 0.5, tp, n_tp)
    drain()
    drain_mixer()
    for copy in copies:
        copy.wait_send()


def spaced(tree):
    if isinstance(tree, dict):
        return SimpleNamespace(**{name: spaced(leaf) for name, leaf in tree.items()})
    return tree


def call_kernel(kernel, inputs, outputs, scratch, name, call_id):
    arrays = [array for array, _ in inputs.values()]
    leaves, tree = jax.tree.flatten(scratch)

    def entry(*given):
        io = dict(zip([*inputs, *outputs], given))
        kernel(spaced(io), spaced(jax.tree.unflatten(tree, given[len(io) :])))

    return pl.pallas_call(
        entry,
        out_shape=[shape for shape, _ in outputs.values()],
        in_specs=[pl.BlockSpec(memory_space=space) for _, space in inputs.values()],
        out_specs=[pl.BlockSpec(memory_space=space) for _, space in outputs.values()],
        scratch_shapes=leaves,
        name=name,
        compiler_params=pltpu.CompilerParams(
            collective_id=call_id, has_side_effects=True, vmem_limit_bytes=LIMIT
        ),
    )(*arrays)


def row_scratch(scratch, rows, block_cols, n):
    scratch.scaled = pltpu.VMEM((rows, block_cols), jnp.bfloat16)
    scratch.row_scale = pltpu.VMEM((rows // n, LANES), jnp.float32)
    scratch.total = pltpu.VMEM((rows, block_cols), jnp.float32)
    return vars(scratch)


def layer(
    x,
    previous_state,
    lengths,
    gain_one,
    w_gate_one,
    w_up_one,
    w_down_one,
    gain_mix,
    w_query,
    w_key,
    w_value,
    w_gate,
    w_beta,
    w_decay,
    decay_rate,
    decay_bias,
    span_bias,
    extra,
    head_gain,
    w_mix,
    gain_two,
    w_gate_two,
    w_up_two,
    w_down_two,
    aligned,
):
    n, n_tp = lax.axis_size(KV), lax.axis_size(TP)
    rows = x.shape[0]
    block_cols, columns = w_gate_one.shape
    own = block_cols // n_tp
    block, heads, head_size = previous_state.shape[:3]
    all_heads = w_beta.shape[1]
    chunks = chunks_of(columns)
    width = columns // chunks
    vmem, hbm = pltpu.VMEM, pltpu.HBM

    def far(array):
        return (pltpu.with_memory_space_constraint(array, hbm), hbm)

    def row(array):
        return array.reshape(1, -1)

    small = dict(
        gain_one=row(gain_one),
        gain_mix=row(gain_mix),
        gain_two=row(gain_two),
        lengths=row(lengths),
        span_bias=span_bias,
        extra=extra.T,
        head_gain=row(head_gain),
        decay_rate=row(decay_rate),
        decay_bias=row(decay_bias),
    )
    inputs = dict(
        x=far(x),
        w_gate_one=far(w_gate_one),
        w_up_one=far(w_up_one),
        w_down_one=far(w_down_one),
        w_query=far(w_query),
        w_key=far(w_key),
        w_value=far(w_value),
        w_gate=far(w_gate),
        w_beta=far(w_beta.T),
        w_decay=far(w_decay.T),
        w_mix=far(w_mix),
        w_gate_two=far(w_gate_two),
        w_up_two=far(w_up_two),
        w_down_two=far(w_down_two),
        previous=far(previous_state),
        **{name: far(array) for name, array in small.items()},
    )
    shape = (rows, own) if aligned else (2, rows // 2, block_cols)
    rows_of_heads = jax.ShapeDtypeStruct((block, heads, head_size), jnp.float32)
    outputs = dict(
        out=(jax.ShapeDtypeStruct(shape, jnp.bfloat16), vmem),
        decays=(rows_of_heads, vmem),
        keys=(rows_of_heads, vmem),
        writes=(rows_of_heads, vmem),
    )
    feed = exchange_scratch(n, chunks, rows, 2 * width, width, (8, LANES))
    feed.weights = vmem((chunks, block_cols, 2 * width), jnp.bfloat16)
    feed.down = vmem((chunks, width, block_cols), jnp.bfloat16)
    feed.weight_sem = pltpu.SemaphoreType.DMA((3, chunks))
    mix = exchange_scratch(n, heads, rows, 4 * head_size, head_size, (block, LANES))
    mix.weights = vmem((heads, block_cols, 4 * head_size), jnp.bfloat16)
    mix.mix_out = vmem((heads, head_size, block_cols), jnp.bfloat16)
    mix.weight_sem = pltpu.SemaphoreType.DMA((5, heads))
    mix.state = vmem((min(heads, 4), block, head_size, head_size), jnp.float32)
    mix.state_sem = pltpu.SemaphoreType.DMA((heads,))
    mix.small_weights = vmem((2, all_heads, block_cols), jnp.bfloat16)
    mix.small_sem = pltpu.SemaphoreType.DMA((2,))
    mix.small = vmem((rows, LANES), jnp.float32)
    mix.decay = vmem((heads, block, LANES), jnp.float32)
    mix.beta = vmem((heads, block, LANES), jnp.float32)
    mix.key = vmem((block, head_size), jnp.float32)
    mix.value = vmem((block, head_size), jnp.float32)
    mix.match = vmem((block, head_size), jnp.float32)
    mix.readout = vmem((block, head_size), jnp.float32)
    mix.turned = vmem((head_size, 4 * block), jnp.float32)
    scratch = dict(
        feed=row_scratch(feed, rows, block_cols, n),
        mix=row_scratch(mix, rows, block_cols, n),
        blocks=vmem((3, 2, rows // 2, block_cols), jnp.bfloat16),
        sums_one=tp_scratch(n_tp, rows, block_cols),
        sums_mix=tp_scratch(n_tp, rows, block_cols),
        small={name: vmem(array.shape, array.dtype) for name, array in small.items()},
        small_sem=pltpu.SemaphoreType.DMA((len(small),)),
        x_sem=pltpu.SemaphoreType.DMA((2,)),
    )
    if aligned:
        scratch.update(
            pieces=vmem((n_tp, rows, own), jnp.bfloat16),
            piece_sem=pltpu.SemaphoreType.DMA((2, n_tp - 1)),
            out_part=vmem((n_tp, rows, own), jnp.bfloat16),
            out_slot=vmem((n_tp - 1, rows, own), jnp.bfloat16),
            out_sem=pltpu.SemaphoreType.DMA((2, n_tp - 1)),
        )
    else:
        scratch.update(sums_two=tp_scratch(n_tp, rows, block_cols))
    out, decays, keys, writes = call_kernel(
        functools.partial(layer_kernel, gain_one.shape[0], aligned),
        inputs,
        outputs,
        scratch,
        "layer",
        0,
    )
    return out if aligned else out.reshape(rows, block_cols), decays, keys, writes


def body(
    tokens,
    previous_state,
    lengths,
    first_feed_norm_gain,
    first_gate_projection,
    first_up_projection,
    first_down_projection,
    mixer_norm_gain,
    query_weight,
    key_weight,
    value_weight,
    output_gate_weight,
    write_strength_weight,
    decay_input_weight,
    head_log_decay_rate,
    decay_input_bias,
    length_span_bias,
    extra_log_decay,
    readout_head_norm_gain,
    mixer_output_weight,
    second_feed_norm_gain,
    second_gate_projection,
    second_up_projection,
    second_down_projection,
):
    own_cols = tokens.shape[1]
    aligned = own_cols % LANES == 0
    if not aligned:
        tokens = lax.all_gather(tokens, TP, axis=1, tiled=True)
    result, decays, keys, writes = layer(
        tokens,
        previous_state,
        lengths,
        first_feed_norm_gain,
        first_gate_projection,
        first_up_projection,
        first_down_projection,
        mixer_norm_gain,
        query_weight,
        key_weight,
        value_weight,
        output_gate_weight,
        write_strength_weight,
        decay_input_weight,
        head_log_decay_rate,
        decay_input_bias,
        length_span_bias,
        extra_log_decay,
        readout_head_norm_gain,
        mixer_output_weight,
        second_feed_norm_gain,
        second_gate_projection,
        second_up_projection,
        second_down_projection,
        aligned,
    )
    new_state = (
        decays[:, :, None, :] * previous_state + keys[:, :, :, None] * writes[:, :, None, :]
    )
    if not aligned:
        start = lax.axis_index(TP) * own_cols
        result = lax.dynamic_slice_in_dim(result, start, own_cols, 1)
    return (result, new_state)


def solution(mesh):
    return jax.shard_map(
        body,
        mesh=mesh,
        in_specs=(
            P(None, (KV, TP)),
            P(KV, TP, None, None),
            P(KV),
            P(),
            P(KV, TP),
            P(KV, TP),
            P(TP, KV),
            P(),
            P(KV, TP),
            P(KV, TP),
            P(KV, TP),
            P(KV, TP),
            P(),
            P(),
            P(TP),
            P(TP),
            P(TP, None),
            P(KV, TP),
            P(),
            P(TP, KV),
            P(),
            P(KV, TP),
            P(KV, TP),
            P(TP, KV),
        ),
        out_specs=(P(None, (KV, TP)), P(KV, TP, None, None)),
        check_vma=False,
    )
```
